128 devices in a mesh: fs: 16 (over z, y), tp: 8 (over x, core).
Axes of the slice: x: 4, y: 4, z: 4, core: 2. Of those that a mesh axis runs over, the one named last changes fastest.
Arguments:
- tokens: bfloat16 [16384, 2048], P(('fs', 'tp')), may hold values from -6 to 6
- first_block_norm_scale: float32 [2048], replicated, may hold values from 0.1 to 1.9
- first_block_gate_matrix: bfloat16 [2048, 5504], P('fs', 'tp'), may hold values from -0.125 to 0.125
- first_block_up_matrix: bfloat16 [2048, 5504], P('fs', 'tp'), may hold values from -0.125 to 0.125
- first_block_down_matrix: bfloat16 [5504, 2048], P('tp', 'fs'), may hold values from -0.078125 to 0.078125
- mixer_norm_scale: float32 [2048], replicated, may hold values from 0.1 to 1.9
- recurrent_input_matrix: bfloat16 [2048, 3072], P('fs', 'tp'), may hold values from -0.125 to 0.125
- output_gate_projection: bfloat16 [2048, 3072], P('fs', 'tp'), may hold values from -0.125 to 0.125
- convolution_kernel: float32 [4, 3072], P(None, 'tp'), may hold values from -2 to 2
- decay_gate_blocks: bfloat16 [16, 192, 192], P('tp'), may hold values from -0.4375 to 0.4375
- input_gate_blocks: bfloat16 [16, 192, 192], P('tp'), may hold values from -0.4375 to 0.4375
- channel_decay_weight: float32 [3072], P('tp'), may hold values from 3.5 to 11.5
- position_decay_extra: float32 [16384], P('fs'), may hold values from -0.7 to 0
- mixer_output_matrix: bfloat16 [3072, 2048], P('tp', 'fs'), may hold values from -0.109375 to 0.109375
- second_block_norm_scale: float32 [2048], replicated, may hold values from 0.1 to 1.9
- second_block_gate_matrix: bfloat16 [2048, 5504], P('fs', 'tp'), may hold values from -0.125 to 0.125
- second_block_up_matrix: bfloat16 [2048, 5504], P('fs', 'tp'), may hold values from -0.125 to 0.125
- second_block_down_matrix: bfloat16 [5504, 2048], P('tp', 'fs'), may hold values from -0.078125 to 0.078125
Outputs:
- layer_out: bfloat16 [16384, 2048], P(('fs', 'tp'))
The draws below stay inside these ranges and needn't reach their ends.
All inputs are finite; a program needn't handle non-finite values.
Results may differ from the reference program's by a relative error of at most 0.019.
Values may be sent and summed in bfloat16 or wider, within the bound.
No kernel may reach another device: no remote copies, remote signals or barrier semaphores. Data moves between devices by JAX's collectives and lax.ppermute only.
A program may use at most 128 MiB of HBM per device.

```python
import jax
import jax.numpy as jnp
from jax import lax

D = 2048
FF = 5504
DR = 3072
RB = 16
BLK = 192
CONV = 4
SEQUENCE_TOKENS = 1024
TOKENS = 16384
N_TP = 8


def draw_channel_decay_weight(key, part):
    pick_key = jax.random.fold_in(key, 11)
    slow_key = jax.random.fold_in(key, 12)
    quick_key = jax.random.fold_in(key, 13)
    fraction = 0.5
    quick_mask = jax.random.bernoulli(pick_key, fraction, (DR,))
    slow_log = jax.random.uniform(slow_key, (DR,), jnp.float32, minval=jnp.log(2e-05), maxval=jnp.log(0.00025))
    quick_log = jax.random.uniform(quick_key, (DR,), jnp.float32, minval=jnp.log(0.004), maxval=jnp.log(0.02))
    softened = jnp.exp(jnp.where(quick_mask, quick_log, slow_log))
    return (-jnp.log(jnp.expm1(softened))).astype(jnp.float32)


def draw_position_decay_extra(key, part):
    where_key = jax.random.fold_in(key, 21)
    depth_key = jax.random.fold_in(key, 22)
    struck = jax.random.bernoulli(where_key, 4.0 / SEQUENCE_TOKENS, (TOKENS,))
    strength = jax.random.uniform(depth_key, (TOKENS,), jnp.float32, minval=jnp.log(0.5), maxval=jnp.log(0.8))
    return jnp.where(struck, strength, 0.0).astype(jnp.float32)


def block_scale(rng, dims, cuts, least, largest):
    def one(dim, parts):
        draws = jax.random.uniform(jax.random.fold_in(jax.random.fold_in(rng, 6), dim), (parts,), jnp.float32, least / len(cuts), largest / len(cuts))
        return jnp.repeat(jnp.exp(draws), dims[dim] // parts).reshape((-1,) + (1,) * (len(dims) - dim - 1))

    level = one(*cuts[0])
    for cut in cuts[1:]:
        level = level * one(*cut)
    return level


def centred(own_key, dims, spread, reach, cuts=(), dtype=jnp.bfloat16):
    loudness = block_scale(own_key, dims, cuts, -0.22, 0.18) if cuts else 1.0
    values = jax.random.normal(own_key, dims, jnp.float32) * spread * loudness
    return jnp.minimum(jnp.maximum(values, -reach), reach).astype(dtype)


def setup_inputs(seed: int = 0) -> dict:
    arg_keys = jax.random.split(jax.random.key(seed), 19)
    return {
        "tokens": centred(arg_keys[0], (TOKENS, D), 1.0, 6.0, ((0, 128),)),
        "first_block_norm_scale": jnp.clip(1.0 + 0.18 * jax.random.normal(arg_keys[1], (D,), jnp.float32), 0.1, 1.9),
        "first_block_gate_matrix": centred(arg_keys[2], (D, FF), D ** -0.5, 0.125, ((0, 16), (1, 8))),
        "first_block_up_matrix": centred(arg_keys[3], (D, FF), D ** -0.5, 0.125, ((0, 16), (1, 8))),
        "first_block_down_matrix": centred(arg_keys[4], (FF, D), FF ** -0.5, 0.078125, ((0, 8), (1, 16))),
        "mixer_norm_scale": jnp.clip(1.0 + 0.18 * jax.random.normal(arg_keys[5], (D,), jnp.float32), 0.1, 1.9),
        "recurrent_input_matrix": centred(arg_keys[6], (D, DR), D ** -0.5, 0.125, ((0, 16), (1, 8))),
        "output_gate_projection": centred(arg_keys[7], (D, DR), D ** -0.5, 0.125, ((0, 16), (1, 8))),
        "convolution_kernel": centred(arg_keys[8], (CONV, DR), 0.5, 2.0, ((1, 8),), jnp.float32),
        "decay_gate_blocks": centred(arg_keys[9], (RB, BLK, BLK), BLK ** -0.5, 0.4375, ((0, 8),)),
        "input_gate_blocks": centred(arg_keys[10], (RB, BLK, BLK), BLK ** -0.5, 0.4375, ((0, 8),)),
        "channel_decay_weight": draw_channel_decay_weight(jax.random.fold_in(arg_keys[18], 71), 0),
        "position_decay_extra": draw_position_decay_extra(jax.random.fold_in(arg_keys[18], 71), 0),
        "mixer_output_matrix": centred(arg_keys[13], (DR, D), DR ** -0.5, 0.109375, ((0, 8), (1, 16))),
        "second_block_norm_scale": jnp.clip(1.0 + 0.18 * jax.random.normal(arg_keys[14], (D,), jnp.float32), 0.1, 1.9),
        "second_block_gate_matrix": centred(arg_keys[15], (D, FF), D ** -0.5, 0.125, ((0, 16), (1, 8))),
        "second_block_up_matrix": centred(arg_keys[16], (D, FF), D ** -0.5, 0.125, ((0, 16), (1, 8))),
        "second_block_down_matrix": centred(arg_keys[17], (FF, D), FF ** -0.5, 0.078125, ((0, 8), (1, 16))),
    }


EPS = 1e-06
RECURRENT_WIDTH = 8.0

def normed(input_token_rows, norm_scale_vector):
    values = input_token_rows.astype(jnp.float32)
    square = lax.optimization_barrier(jnp.mean(values * values, axis=-1, keepdims=True))
    return (values * lax.rsqrt(square + EPS) * norm_scale_vector).astype(jnp.bfloat16)

def block_sum(hidden, weight):
    span_width = hidden.shape[1] // N_TP
    running = jnp.zeros((hidden.shape[0], weight.shape[1]), jnp.float32)
    for index_k in range(N_TP):
        lower = index_k * span_width
        partial_sum = jnp.dot(hidden[:, lower:lower + span_width], weight[lower:lower + span_width], preferred_element_type=jnp.float32).astype(jnp.bfloat16)
        partial_sum = lax.optimization_barrier(partial_sum)
        running = running + partial_sum.astype(jnp.float32)
    return running

def feed_forward(input_token_rows, norm_scale_vector, gate_weight, up_weight, down_weight):
    normal = normed(input_token_rows, norm_scale_vector)
    gate_pre = jnp.dot(normal, gate_weight, preferred_element_type=jnp.float32)
    up_pre = jnp.dot(normal, up_weight, preferred_element_type=jnp.float32)
    hidden = (jax.nn.silu(gate_pre) * up_pre).astype(jnp.bfloat16)
    return block_sum(hidden, down_weight)

def blockwise(values, weight):
    dims_in = values.shape
    grouped = values.reshape(dims_in[:-1] + (weight.shape[0], weight.shape[1])).astype(jnp.float32)
    result = jnp.einsum('sthi,hij->sthj', grouped, weight.astype(jnp.float32))
    return result.reshape(dims_in)

def combine(earlier, later):
    decay_one, drive_one = earlier
    decay_two, drive_two = later
    return (decay_one * decay_two, decay_two * drive_one + drive_two)

def linear_recurrence_scan(input_token_rows, norm_scale_vector, recurrent_input_matrix, output_gate_projection, convolution_kernel, decay_gate_blocks, input_gate_blocks, channel_decay_weight, position_decay_extra, mixer_output_matrix):
    normal = normed(input_token_rows, norm_scale_vector)
    sequence_batch_count = normal.shape[0] // SEQUENCE_TOKENS
    recur_rows = jnp.dot(normal, recurrent_input_matrix, preferred_element_type=jnp.float32).astype(jnp.bfloat16)
    branch_rows = jnp.dot(normal, output_gate_projection, preferred_element_type=jnp.float32).astype(jnp.bfloat16)
    recur_rows = recur_rows.reshape(sequence_batch_count, SEQUENCE_TOKENS, -1)
    branch_rows = branch_rows.reshape(sequence_batch_count, SEQUENCE_TOKENS, -1)
    taps = convolution_kernel.shape[0]
    padded = jnp.pad(recur_rows, ((0, 0), (taps - 1, 0), (0, 0)))
    summed = jnp.zeros(recur_rows.shape, jnp.float32)
    for offset in range(taps):
        summed = summed + padded[:, offset:offset + SEQUENCE_TOKENS].astype(jnp.float32) * convolution_kernel[offset]
    conv_out = summed.astype(jnp.bfloat16)
    decay_gate_value = jax.nn.sigmoid(blockwise(conv_out, decay_gate_blocks))
    input_gate = jax.nn.sigmoid(blockwise(conv_out, input_gate_blocks))
    log_decay_factor = -RECURRENT_WIDTH * decay_gate_value * jax.nn.softplus(-channel_decay_weight) + position_decay_extra.reshape(sequence_batch_count, SEQUENCE_TOKENS, 1)
    decay_rate = jnp.exp(log_decay_factor)
    drive_in = jnp.sqrt(-jnp.expm1(2.0 * log_decay_factor)) * input_gate * conv_out.astype(jnp.float32)
    _, hidden_state = lax.associative_scan(combine, (decay_rate, drive_in), axis=1)
    gated = (jax.nn.gelu(branch_rows.astype(jnp.float32), approximate=True) * hidden_state).astype(jnp.bfloat16)
    return block_sum(gated.reshape(sequence_batch_count * SEQUENCE_TOKENS, -1), mixer_output_matrix)

def reference(tokens, first_block_norm_scale, first_block_gate_matrix, first_block_up_matrix, first_block_down_matrix, mixer_norm_scale, recurrent_input_matrix, output_gate_projection, convolution_kernel, decay_gate_blocks, input_gate_blocks, channel_decay_weight, position_decay_extra, mixer_output_matrix, second_block_norm_scale, second_block_gate_matrix, second_block_up_matrix, second_block_down_matrix):
    first_out = feed_forward(tokens, first_block_norm_scale, first_block_gate_matrix, first_block_up_matrix, first_block_down_matrix)
    residual_activations = (tokens.astype(jnp.float32) + 0.5 * first_out).astype(jnp.bfloat16)
    mixer_output_rows = linear_recurrence_scan(residual_activations, mixer_norm_scale, recurrent_input_matrix, output_gate_projection, convolution_kernel, decay_gate_blocks, input_gate_blocks, channel_decay_weight, position_decay_extra, mixer_output_matrix)
    residual_activations = (residual_activations.astype(jnp.float32) + mixer_output_rows).astype(jnp.bfloat16)
    second_out = feed_forward(residual_activations, second_block_norm_scale, second_block_gate_matrix, second_block_up_matrix, second_block_down_matrix)
    return (residual_activations.astype(jnp.float32) + 0.5 * second_out).astype(jnp.bfloat16)
```

```python
import functools

import jax
import jax.numpy as jnp
from jax import lax
from jax.experimental import pallas as pl
from jax.experimental.pallas import tpu as pltpu
from jax.sharding import PartitionSpec as P


EPS = 1e-06
RECURRENT_WIDTH = 8.0
BF = jnp.bfloat16
F32 = jnp.float32
LANE = 128
VMEM_LIMIT = 60 * 1024 * 1024


def along_tp(value, step, other_core):
    chips = lax.axis_size("tp") // 2
    pairs = [
        (x * 2 + c, ((x + step) % chips) * 2 + (c ^ other_core))
        for x in range(chips)
        for c in range(2)
    ]
    return lax.ppermute(value, "tp", pairs)


def spread_rows(top, bottom):
    prev_top = along_tp(top, 1, 0)
    next_bottom = along_tp(bottom, -1, 0)
    prev_bottom = along_tp(bottom, 1, 0)
    next_top = along_tp(top, -1, 0)
    far_top = along_tp(prev_top, 1, 0)
    far_bottom = along_tp(next_bottom, -1, 0)
    same = [far_top, far_bottom, next_top, next_bottom, prev_top, prev_bottom, top, bottom]
    other = [along_tp(v, 0, 1) for v in same]
    return same + other


def add(a, b):
    return (a.astype(F32) + b.astype(F32)).astype(BF)


def collect_rows(same_far, same_near, other_far, other_near):
    got_far = along_tp(other_far, 0, 1)
    got_near = along_tp(other_near, 0, 1)
    rows = same_far.shape[0]
    half = rows // 2
    far = add(same_far, got_far)
    via_next = along_tp(far[:half], 1, 0)
    via_prev = along_tp(far[half:], -1, 0)
    near = same_near.astype(F32) + got_near.astype(F32)
    to_next = near[:rows]
    to_prev = near[rows : 2 * rows]
    to_next = jnp.concatenate([to_next[:half] + via_next.astype(F32), to_next[half:]], 0)
    to_prev = jnp.concatenate([to_prev[:half], to_prev[half:] + via_prev.astype(F32)], 0)
    from_prev = along_tp(to_next.astype(BF), 1, 0)
    from_next = along_tp(to_prev.astype(BF), -1, 0)
    return near[2 * rows :] + from_prev.astype(F32) + from_next.astype(F32)


def pack_feed(gate_ref, up_ref, down_ref, out_ref):
    width = gate_ref.shape[1]
    rows = gate_ref.shape[0]
    whole = width // LANE
    rest = width - whole * LANE
    for j in range(whole):
        out_ref[pl.ds(2 * j * rows, rows), :] = gate_ref[:, j * LANE : (j + 1) * LANE]
        out_ref[pl.ds((2 * j + 1) * rows, rows), :] = up_ref[:, j * LANE : (j + 1) * LANE]
    gap = jnp.zeros((rows, LANE // 2 - rest), BF)
    out_ref[pl.ds(2 * whole * rows, rows), :] = jnp.concatenate(
        [gate_ref[:, whole * LANE :], gap, up_ref[:, whole * LANE :], gap], axis=1
    )
    at = (2 * whole + 1) * rows
    out_ref[pl.ds(at, width), :] = down_ref[...]
    pad = out_ref.shape[0] - at - width
    out_ref[pl.ds(at + width, pad), :] = jnp.zeros((pad, LANE), BF)


def pack_mixer(first_ref, second_ref, out_w_ref, out_ref):
    rows = first_ref.shape[0]
    blocks = first_ref.shape[1] // LANE
    for j in range(blocks):
        out_ref[pl.ds(j * rows, rows), :] = first_ref[:, j * LANE : (j + 1) * LANE]
        out_ref[pl.ds((blocks + j) * rows, rows), :] = second_ref[:, j * LANE : (j + 1) * LANE]
    out_ref[pl.ds(2 * blocks * rows, out_w_ref.shape[0]), :] = out_w_ref[...]


def packed(kernel, first, second, third, length):
    return pl.pallas_call(
        kernel,
        out_shape=jax.ShapeDtypeStruct((length, LANE), BF),
        name=kernel.__name__,
    )(first, second, third)


def load_rows(pieces, x_ref, sem, starts):
    copies = []
    for i, piece in enumerate(pieces):
        copies.append(
            pltpu.make_async_copy(piece, x_ref.at[pl.ds(starts[i], piece.shape[0])], sem.at[i])
        )
    return copies


def feed_body(*refs, rows, hidden, model):
    pieces = refs[:16]
    w_ref = refs[16]
    outs = refs[17:21]
    x_ref, w_in, w_out, h_ref, y_ref, x_sem, w_sem, o_sem = refs[21:]
    fs = w_ref.shape[0]
    half = rows // 2
    whole = hidden // LANE
    rest = hidden - whole * LANE
    kin = LANE
    steps = whole + 1
    wide = 2 * LANE
    total = x_ref.shape[0]

    row_copies = load_rows(pieces, x_ref, x_sem, [i * half for i in range(16)])
    w_copies = []
    for j in range(steps):
        n = wide if j < whole else LANE
        w_copies.append(
            pltpu.make_async_copy(
                w_ref.at[:, pl.ds(j * wide, n), :], w_in.at[:, pl.ds(j * wide, n), :], w_sem.at[j]
            )
        )
    down_at = (2 * whole + 1) * kin
    down = pltpu.make_async_copy(
        w_ref.at[:, pl.ds(down_at, w_out.shape[1]), :], w_out, w_sem.at[steps]
    )
    w_copies[0].start()
    for c in row_copies:
        c.start()
    for c in w_copies[1:]:
        c.start()
    down.start()
    for c in row_copies:
        c.wait()

    chunk = min(512, total)
    loops = total // chunk

    for j in range(steps):
        w_copies[j].wait()
        if j < whole:
            gate = w_in[:, j * wide : j * wide + LANE, :].reshape(fs * LANE, LANE)
            up = w_in[:, j * wide + LANE : (j + 1) * wide, :].reshape(fs * LANE, LANE)
            weight = jnp.concatenate([gate, up], axis=1)
        else:
            weight = w_in[:, j * wide : j * wide + LANE, :].reshape(fs * LANE, LANE)

        for m in range(loops):
            x = x_ref[pl.ds(m * chunk, chunk), :]
            both = jnp.dot(x, weight, preferred_element_type=F32)
            if j < whole:
                gate_pre = both[:, :LANE]
                up_pre = both[:, LANE:]
                hid = gate_pre / (1.0 + jnp.exp(-gate_pre)) * up_pre
            else:
                up_pre = pltpu.roll(both, LANE // 2, 1)
                lane = lax.broadcasted_iota(jnp.int32, both.shape, 1)
                hid = jnp.where(lane < rest, both / (1.0 + jnp.exp(-both)) * up_pre, 0.0)
            h_ref[pl.ds(m * chunk, chunk), j * LANE : (j + 1) * LANE] = hid.astype(BF)

    down.wait()
    out_rows = w_out.shape[1]
    o_copies = []
    for f in range(fs // 2):
        weight = jnp.concatenate([w_out[2 * f], w_out[2 * f + 1]], axis=1)
        for m in range(loops):
            h = h_ref[pl.ds(m * chunk, chunk), :out_rows]
            y = jnp.dot(h, weight, preferred_element_type=F32)
            y_ref[pl.ds(m * chunk, chunk), f * wide : (f + 1) * wide] = y.astype(BF)
        at = 0
        for i, out in enumerate(outs):
            copy = pltpu.make_async_copy(
                y_ref.at[pl.ds(at, out.shape[0]), f * wide : (f + 1) * wide],
                out.at[:, f * wide : (f + 1) * wide],
                o_sem.at[f, i],
            )
            copy.start()
            o_copies.append(copy)
            at += out.shape[0]
    for copy in o_copies:
        copy.wait()


def feed_call(pieces, weights, rows, hidden):
    model = pieces[0].shape[1]
    fs = model // LANE
    length = weights.shape[0] // fs
    weights = weights.reshape(fs, length, LANE)
    total = rows * 8
    whole = hidden // LANE
    in_rows = (2 * whole + 1) * LANE
    out_rows = length - in_rows
    body = functools.partial(feed_body, rows=rows, hidden=hidden, model=model)
    shapes = [(rows, model), (3 * rows, model), (rows, model), (3 * rows, model)]
    flops = 2 * total * model * (in_rows + out_rows)
    return pl.pallas_call(
        body,
        in_specs=[pl.BlockSpec(memory_space=pl.ANY)] * 17,
        out_specs=[pl.BlockSpec(memory_space=pl.ANY)] * 4,
        out_shape=[jax.ShapeDtypeStruct(s, BF) for s in shapes],
        scratch_shapes=[
            pltpu.VMEM((total, model), BF),
            pltpu.VMEM((fs, in_rows, LANE), BF),
            pltpu.VMEM((fs, out_rows, LANE), BF),
            pltpu.VMEM((total, (whole + 1) * LANE), BF),
            pltpu.VMEM((total, model), BF),
            pltpu.SemaphoreType.DMA((16,)),
            pltpu.SemaphoreType.DMA((whole + 2,)),
            pltpu.SemaphoreType.DMA((fs // 2, 4)),
        ],
        compiler_params=pltpu.CompilerParams(vmem_limit_bytes=VMEM_LIMIT),
        cost_estimate=pl.CostEstimate(
            flops=flops, bytes_accessed=2 * total * model * 2, transcendentals=0
        ),
        name="feed",
    )(*pieces, weights)


def mixer_body(*refs, rows, channels):
    starts = refs[0]
    pieces = refs[1:17]
    w_ref, gates_ref, taps_ref, decay_ref, extra_ref = refs[17:22]
    outs = refs[22:26]
    (x_ref, w_in, w_out, r_ref, b_ref, c_ref, a_ref, d_ref, g_ref, y_ref) = refs[26:36]
    x_sem, w_sem, o_sem = refs[36:]
    fs = w_ref.shape[0]
    half = rows // 2
    total = x_ref.shape[0]
    wide = 2 * LANE
    blocks = channels // LANE
    pairs = blocks

    at = [pl.multiple_of(starts[i], rows) for i in range(8)]
    where = []
    for i in range(8):
        where += [at[i], at[i] + half]
    row_copies = load_rows(pieces, x_ref, x_sem, where)
    w_copies = [
        pltpu.make_async_copy(
            w_ref.at[:, pl.ds(j * wide, wide), :], w_in.at[:, pl.ds(j * wide, wide), :], w_sem.at[j]
        )
        for j in range(pairs)
    ]
    out_copy = pltpu.make_async_copy(
        w_ref.at[:, pl.ds(pairs * wide, channels), :], w_out, w_sem.at[pairs]
    )
    w_copies[0].start()
    for c in row_copies:
        c.start()
    for c in w_copies[1:]:
        c.start()
    out_copy.start()
    for c in row_copies:
        c.wait()

    chunk = min(512, total)
    loops = total // chunk
    pad = 8
    r_ref[:pad, :] = jnp.zeros((pad, channels), F32)
    for j in range(pairs):
        w_copies[j].wait()
        weight = jnp.concatenate(
            [
                w_in[:, j * wide : j * wide + LANE, :].reshape(fs * LANE, LANE),
                w_in[:, j * wide + LANE : (j + 1) * wide, :].reshape(fs * LANE, LANE),
            ],
            axis=1,
        )
        for m in range(loops):
            both = jnp.dot(x_ref[pl.ds(m * chunk, chunk), :], weight, preferred_element_type=F32)
            for k in range(2):
                block = 2 * j + k
                value = both[:, k * LANE : (k + 1) * LANE].astype(BF).astype(F32)
                if block < blocks:
                    r_ref[pl.ds(pad + m * chunk, chunk), block * LANE : (block + 1) * LANE] = value
                else:
                    block -= blocks
                    b_ref[pl.ds(m * chunk, chunk), block * LANE : (block + 1) * LANE] = value

    taps = taps_ref.shape[0]
    step = 128
    for m in range(total // step):
        base = m * step
        acc = r_ref[pl.ds(base + pad - taps + 1, step), :] * taps_ref[0:1, :]
        for j in range(1, taps):
            acc = acc + r_ref[pl.ds(base + pad - taps + 1 + j, step), :] * taps_ref[j : j + 1, :]
        c_ref[pl.ds(base, step), :] = acc.astype(BF)

    decay = decay_ref[...]

    def gates(m, carry):
        base = pl.multiple_of(m * step, step)
        conv = c_ref[pl.ds(base, step), :]
        pre = jnp.dot(conv, gates_ref[...], preferred_element_type=F32)
        sig = 1.0 / (1.0 + jnp.exp(-pre))
        log_a = sig[:, :channels] * decay + extra_ref[pl.ds(base, step), :]
        twice = 2.0 * log_a
        a_val = jnp.exp(log_a)
        series = -twice * (
            1.0
            + twice
            * (0.5 + twice * (1.0 / 6 + twice * (1.0 / 24 + twice * (1.0 / 120 + twice / 720.0))))
        )
        rest = jnp.where(twice > -0.25, series, 1.0 - jnp.exp(twice))
        drive = jnp.sqrt(rest) * sig[:, channels:] * conv.astype(F32)
        a_ref[pl.ds(base, step), :] = a_val
        d_ref[pl.ds(base, step), :] = drive
        return carry

    lax.fori_loop(0, total // step, gates, 0)

    tile = 8
    group = 64
    row_in_tile = lax.broadcasted_iota(jnp.int32, (tile, channels), 0)

    def scan(m, carry):
        base = pl.multiple_of(m * group, group)
        for k in range(group // tile):
            a = a_ref[pl.ds(base + k * tile, tile), :]
            d = d_ref[pl.ds(base + k * tile, tile), :]
            for shift in (1, 2, 4):
                keep = row_in_tile >= shift
                a_prev = jnp.where(keep, pltpu.roll(a, shift, 0), 1.0)
                d_prev = jnp.where(keep, pltpu.roll(d, shift, 0), 0.0)
                d = a * d_prev + d
                a = a * a_prev
            state = a * carry + d
            carry = jnp.broadcast_to(state[tile - 1 : tile, :], (tile, channels))
            d_ref[pl.ds(base + k * tile, tile), :] = state
        return carry

    lax.fori_loop(0, total // group, scan, jnp.zeros((tile, channels), F32))

    def gating(m, carry):
        base = pl.multiple_of(m * step, step)
        v = b_ref[pl.ds(base, step), :]
        inner = 0.7978845608028654 * (v + 0.044715 * (v * v * v))
        gelu = 0.5 * v * (1.0 + jnp.tanh(inner))
        g_ref[pl.ds(base, step), :] = (gelu * d_ref[pl.ds(base, step), :]).astype(BF)
        return carry

    lax.fori_loop(0, total // step, gating, 0)

    out_copy.wait()
    o_copies = []
    for f in range(fs // 2):
        weight = jnp.concatenate([w_out[2 * f], w_out[2 * f + 1]], axis=1)
        for m in range(loops):
            y = jnp.dot(g_ref[pl.ds(m * chunk, chunk), :], weight, preferred_element_type=F32)
            y_ref[pl.ds(m * chunk, chunk), f * wide : (f + 1) * wide] = y.astype(BF)
        for i in range(8):
            out = outs[2 * (i // 4) + (0 if i % 4 == 0 else 1)]
            to = 0 if i % 4 == 0 else (i % 4 - 1) * rows
            copy = pltpu.make_async_copy(
                y_ref.at[pl.ds(at[i], rows), f * wide : (f + 1) * wide],
                out.at[pl.ds(to, rows), f * wide : (f + 1) * wide],
                o_sem.at[f, i],
            )
            copy.start()
            o_copies.append(copy)
    for copy in o_copies:
        copy.wait()


def mixer_call(starts, pieces, weights, gates, taps, decay, extra, rows):
    model = pieces[0].shape[1]
    channels = taps.shape[1]
    fs = model // LANE
    length = weights.shape[0] // fs
    weights = weights.reshape(fs, length, LANE)
    total = rows * 8
    body = functools.partial(mixer_body, rows=rows, channels=channels)
    shapes = [(rows, model), (3 * rows, model), (rows, model), (3 * rows, model)]
    hbm = pl.BlockSpec(memory_space=pl.ANY)
    vmem = pl.BlockSpec(memory_space=pltpu.VMEM)
    flops = 2 * total * model * length
    return pl.pallas_call(
        body,
        in_specs=[pl.BlockSpec(memory_space=pltpu.SMEM)] + [hbm] * 17 + [vmem] * 4,
        out_specs=[hbm] * 4,
        out_shape=[jax.ShapeDtypeStruct(s, BF) for s in shapes],
        scratch_shapes=[
            pltpu.VMEM((total, model), BF),
            pltpu.VMEM((fs, length - channels, LANE), BF),
            pltpu.VMEM((fs, channels, LANE), BF),
            pltpu.VMEM((total + 8, channels), F32),
            pltpu.VMEM((total, channels), F32),
            pltpu.VMEM((total, channels), BF),
            pltpu.VMEM((total, channels), F32),
            pltpu.VMEM((total, channels), F32),
            pltpu.VMEM((total, channels), BF),
            pltpu.VMEM((total, model), BF),
            pltpu.SemaphoreType.DMA((16,)),
            pltpu.SemaphoreType.DMA((channels // LANE + 1,)),
            pltpu.SemaphoreType.DMA((fs // 2, 8)),
        ],
        compiler_params=pltpu.CompilerParams(vmem_limit_bytes=VMEM_LIMIT),
        cost_estimate=pl.CostEstimate(
            flops=flops, bytes_accessed=2 * total * model * 2, transcendentals=0
        ),
        name="mixer",
    )(starts, *pieces, weights, gates, taps, decay, extra)


def normed(values, scale):
    values = values.astype(F32)
    square = jnp.mean(values * values, axis=-1, keepdims=True)
    return (values * lax.rsqrt(square + EPS) * scale).astype(BF)


def halves(x):
    return x[: x.shape[0] // 2], x[x.shape[0] // 2 :]


def block_diagonal(blocks):
    count, size, _ = blocks.shape
    return jnp.concatenate(
        [
            jnp.pad(blocks[b], ((0, 0), (b * size, (count - 1 - b) * size)))
            for b in range(count)
        ],
        axis=0,
    )


def shards(
    tokens,
    first_block_norm_scale,
    first_block_gate_matrix,
    first_block_up_matrix,
    first_block_down_matrix,
    mixer_norm_scale,
    recurrent_input_matrix,
    output_gate_projection,
    convolution_kernel,
    decay_gate_blocks,
    input_gate_blocks,
    channel_decay_weight,
    position_decay_extra,
    mixer_output_matrix,
    second_block_norm_scale,
    second_block_gate_matrix,
    second_block_up_matrix,
    second_block_down_matrix,
):
    rows = tokens.shape[0]
    hidden = first_block_gate_matrix.shape[1]
    channels = recurrent_input_matrix.shape[1]
    feed_length = (2 * (hidden // LANE) + 1) * LANE + -(-hidden // 64) * 64

    first_weights = lax.all_gather(
        packed(
            pack_feed,
            first_block_gate_matrix,
            first_block_up_matrix,
            first_block_down_matrix,
            feed_length,
        ),
        "fs",
        axis=0,
        tiled=True,
    )
    mixer_weights = lax.all_gather(
        packed(
            pack_mixer,
            recurrent_input_matrix,
            output_gate_projection,
            mixer_output_matrix,
            2 * channels + channels,
        ),
        "fs",
        axis=0,
        tiled=True,
    )
    second_weights = lax.all_gather(
        packed(
            pack_feed,
            second_block_gate_matrix,
            second_block_up_matrix,
            second_block_down_matrix,
            feed_length,
        ),
        "fs",
        axis=0,
        tiled=True,
    )
    gates = jnp.concatenate(
        [block_diagonal(decay_gate_blocks), block_diagonal(input_gate_blocks)], axis=1
    )
    decay = (-RECURRENT_WIDTH * jax.nn.softplus(-channel_decay_weight))[None, :]
    extra = position_decay_extra[:, None]
    place = lax.axis_index("tp")
    chip, core = place // 2, place % 2
    starts = jnp.stack(
        [
            (((chip + step) % 4) * 2 + (core + other) % 2) * rows
            for other in range(2)
            for step in (2, 1, 3, 0)
        ]
    ).astype(jnp.int32)

    pieces = spread_rows(*halves(normed(tokens, first_block_norm_scale)))
    first = collect_rows(*feed_call(pieces, first_weights, rows, hidden))
    x1 = (tokens.astype(F32) + 0.5 * first).astype(BF)

    pieces = spread_rows(*halves(normed(x1, mixer_norm_scale)))
    mixed = collect_rows(
        *mixer_call(
            starts, pieces, mixer_weights, gates, convolution_kernel, decay, extra, rows
        )
    )
    x2 = (x1.astype(F32) + mixed).astype(BF)

    pieces = spread_rows(*halves(normed(x2, second_block_norm_scale)))
    second = collect_rows(*feed_call(pieces, second_weights, rows, hidden))
    return (x2.astype(F32) + 0.5 * second).astype(BF)


def solution(mesh):
    in_specs = (
        P(("fs", "tp"), None),
        P(),
        P("fs", "tp"),
        P("fs", "tp"),
        P("tp", "fs"),
        P(),
        P("fs", "tp"),
        P("fs", "tp"),
        P(None, "tp"),
        P("tp", None, None),
        P("tp", None, None),
        P("tp"),
        P("fs"),
        P("tp", "fs"),
        P(),
        P("fs", "tp"),
        P("fs", "tp"),
        P("tp", "fs"),
    )
    out_specs = P(("fs", "tp"), None)
    return jax.shard_map(shards, mesh=mesh, in_specs=in_specs, out_specs=out_specs, check_vma=False)
```

```python
import functools

import jax
import jax.numpy as jnp
from jax import lax
from jax.experimental import pallas as pl
from jax.experimental.pallas import tpu as pltpu
from jax.sharding import PartitionSpec as P


EPS = 1e-06
RECURRENT_WIDTH = 8.0
BF = jnp.bfloat16
F32 = jnp.float32
LANE = 128
CHUNK = 512
VMEM_LIMIT = 24 * 1024 * 1024


def along_tp(value, step, other_core):
    chips = lax.axis_size("tp") // 2
    pairs = [
        (x * 2 + c, ((x + step) % chips) * 2 + (c ^ other_core))
        for x in range(chips)
        for c in range(2)
    ]
    return lax.ppermute(value, "tp", pairs)


def across(values):
    return [along_tp(v, 0, 1) for v in values]


def after(values, *done):
    return lax.optimization_barrier((values, done))[0]


def spread_near(top, bottom):
    prev_top = along_tp(top, 1, 0)
    next_bottom = along_tp(bottom, -1, 0)
    prev_bottom = along_tp(bottom, 1, 0)
    next_top = along_tp(top, -1, 0)
    return [next_top, next_bottom, prev_top, prev_bottom]


def spread_far(near):
    return [along_tp(near[2], 1, 0), along_tp(near[1], -1, 0)]


def plus(a, b):
    return a.astype(F32) + b.astype(F32)


def send_far(far):
    half = far.shape[0] // 2
    return along_tp(far[:half], 1, 0), along_tp(far[half:], -1, 0)


def near_sums(same, got):
    half = same.shape[0] // 4
    return [plus(same[k * half : (k + 1) * half], got[k * half : (k + 1) * half]) for k in range(4)]


def send_free(near):
    return along_tp(near[1].astype(BF), 1, 0), along_tp(near[2].astype(BF), -1, 0)


def send_rest(near, via):
    return (
        along_tp(plus(near[0], via[0]).astype(BF), 1, 0),
        along_tp(plus(near[3], via[1]).astype(BF), -1, 0),
    )


def own_sums(own, free, rest):
    half = own[0].shape[0] // 2
    return [
        plus(own[0][:half], own[1][:half]) + plus(free[1], rest[0]),
        plus(own[0][half:], own[1][half:]) + plus(free[0], rest[1]),
    ]


def along_fs(value, z_step, y_step):
    side = 4
    pairs = [
        (z * side + y, ((z + z_step) % side) * side + (y + y_step) % side)
        for z in range(side)
        for y in range(side)
    ]
    return lax.ppermute(value, "fs", pairs)


def ring_pieces(value, cut, move):
    prev = move(value, 1)
    nxt = move(value, -1)
    return [value, prev, nxt, move(prev[:cut], 1), move(nxt[cut:], -1)]


def gathered_down(shard):
    rows = shard.shape[0]
    cut = -(-rows // 32) * 16
    row = jnp.concatenate(ring_pieces(shard, cut, lambda v, s: along_fs(v, 0, s)), axis=0)
    return ring_pieces(row, 2 * rows, lambda v, s: along_fs(v, s, 0))


FS_STEPS = [(z, y) for z in (0, -1, 1, 2) for y in (0, -1, 1, 2)]


def pack_in(gate_ref, up_ref, out_ref):
    width, rows = gate_ref.shape
    whole = width // LANE
    rest = width - whole * LANE
    for j in range(whole):
        for k, ref in enumerate((gate_ref, up_ref)):
            block = ref[j * LANE : (j + 1) * LANE, :]
            out_ref[pl.ds((2 * j + k) * rows, rows), :] = block.T
    gap = jnp.zeros((LANE // 2 - rest, rows), BF)
    block = jnp.concatenate(
        [gate_ref[whole * LANE :, :], gap, up_ref[whole * LANE :, :], gap], axis=0
    )
    out_ref[pl.ds(2 * whole * rows, rows), :] = block.T


def pack_feed(gate_ref, up_ref, down_ref, out_ref):
    width, rows = gate_ref.shape
    pack_in(gate_ref, up_ref, out_ref)
    at = (2 * (width // LANE) + 1) * rows
    out_ref[pl.ds(at, width), :] = down_ref[...]


def pack_mixer(first_ref, second_ref, out_w_ref, out_ref):
    rows = first_ref.shape[0]
    blocks = first_ref.shape[1] // LANE
    for j in range(blocks):
        out_ref[pl.ds(j * rows, rows), :] = first_ref[:, j * LANE : (j + 1) * LANE]
        out_ref[pl.ds((blocks + j) * rows, rows), :] = second_ref[:, j * LANE : (j + 1) * LANE]
    out_ref[pl.ds(2 * blocks * rows, out_w_ref.shape[0]), :] = out_w_ref[...]


def packed(kernel, arrays, length):
    return pl.pallas_call(
        kernel,
        out_shape=jax.ShapeDtypeStruct((length, LANE), BF),
        name=kernel.__name__,
    )(*arrays)


def gathered(shard):
    fs = lax.axis_size("fs")
    return lax.all_gather(shard, "fs", axis=0, tiled=True).reshape(fs, -1, LANE)


def load_rows(pieces, x_ref, sem):
    copies = []
    at = 0
    for i, piece in enumerate(pieces):
        rows = piece.shape[0]
        copies.append(pltpu.make_async_copy(piece, x_ref.at[pl.ds(at, rows)], sem.at[i]))
        at += rows
    for c in copies:
        c.start()
    for c in copies:
        c.wait()


HBM = pl.BlockSpec(memory_space=pl.ANY)
VMEM = pl.BlockSpec(memory_space=pltpu.VMEM)
SMEM = pl.BlockSpec(memory_space=pltpu.SMEM)


def call(body, name, outs, scratch, operands, specs, out_specs, flops):
    return pl.pallas_call(
        body,
        in_specs=specs,
        out_specs=out_specs,
        out_shape=outs,
        scratch_shapes=scratch,
        compiler_params=pltpu.CompilerParams(vmem_limit_bytes=VMEM_LIMIT),
        cost_estimate=pl.CostEstimate(flops=flops, bytes_accessed=1 << 20, transcendentals=0),
        name=name,
    )(*operands)


def place_body(*refs, parts, inner):
    places_ref, w_ref = refs[:2]
    down_refs = refs[2 : 2 + parts]
    w_in, w_out, sem = refs[2 + parts :]
    fs = w_in.shape[0]
    blocks = w_in.shape[2] // LANE
    copies = [
        pltpu.make_async_copy(
            w_ref.at[:, pl.ds(j * LANE, LANE), :],
            w_in.at[:, :, pl.ds(j * LANE, LANE)],
            sem.at[0],
        )
        for j in range(blocks)
    ]
    if parts == 0:
        shards = [w_ref.at[f, pl.ds(blocks * LANE, inner), :] for f in range(fs)]
        places = [f * LANE for f in range(fs)]
    else:
        shards = [
            ref.at[pl.ds(i * inner, inner), :]
            for ref in down_refs
            for i in range(ref.shape[0] // inner)
        ]
        places = [pl.multiple_of(places_ref[i], LANE) for i in range(fs)]
    copies += [
        pltpu.make_async_copy(
            shard, w_out.at[pl.ds(0, inner), pl.ds(place, LANE)], sem.at[0]
        )
        for shard, place in zip(shards, places)
    ]
    for c in copies:
        c.start()
    pad = w_out.shape[0] - inner
    if pad:
        w_out[inner:, :] = jnp.zeros((pad, w_out.shape[1]), BF)
    for c in copies:
        c.wait()


def placed(places, weights, downs, blocks, inner):
    fs = weights.shape[0]
    held = -(-inner // LANE) * LANE
    weights, *downs = [pltpu.with_memory_space_constraint(w, pltpu.HBM) for w in (weights, *downs)]
    got = call(
        functools.partial(place_body, parts=len(downs), inner=inner),
        "place",
        [pltpu.VMEM((fs, LANE, blocks * LANE), BF), pltpu.VMEM((held, fs * LANE), BF)],
        [pltpu.SemaphoreType.DMA((1,))],
        (places, weights, *downs),
        [SMEM] + [HBM] * (1 + len(downs)),
        [VMEM, VMEM],
        1 << 31,
    )
    return [pltpu.with_memory_space_constraint(g, pltpu.VMEM) for g in got]


def project(x_ref, w_ref, outs, y_ref, sem, chunk):
    steps = y_ref.shape[0]
    total = x_ref.shape[0]
    wide = y_ref.shape[2]

    def send(f):
        at = 0
        made = []
        for i, out in enumerate(outs):
            made.append(
                pltpu.make_async_copy(
                    y_ref.at[f, pl.ds(at, out.shape[0]), :],
                    out.at[:, pl.ds(pl.multiple_of(f * wide, wide), wide)],
                    sem.at[f, i],
                )
            )
            at += out.shape[0]
        return made

    def one(f, carry):
        columns = pl.ds(pl.multiple_of(f * wide, wide), wide)
        for m in range(total // chunk):
            y_ref[f, m * chunk : (m + 1) * chunk] = jnp.dot(
                x_ref[m * chunk : (m + 1) * chunk, :],
                w_ref[:, columns],
                preferred_element_type=F32,
            ).astype(BF)
        for copy in send(f):
            copy.start()
        return carry

    def finish(f, carry):
        for copy in send(f):
            copy.wait()
        return carry

    lax.fori_loop(0, steps, one, 0)
    lax.fori_loop(0, steps, finish, 0)


def feed_body(*refs, count, hidden):
    pieces = refs[:count]
    w_in, w_out = refs[count : count + 2]
    outs = refs[count + 2 : count + 4]
    x_ref, h_ref, y_ref, x_sem, o_sem = refs[count + 4 :]
    total, model = x_ref.shape
    rest = hidden % LANE
    blocks = w_in.shape[2] // LANE
    chunk = min(CHUNK, total)
    load_rows(pieces, x_ref, x_sem)
    wide = 4 * LANE
    steps = total // chunk

    def silu(v):
        return v / (1.0 + jnp.exp(-v))

    def one(i, carry):
        rows = pl.ds(pl.multiple_of(i % steps * chunk, chunk), chunk)
        group = i // steps
        both = jnp.dot(
            x_ref[rows, :],
            w_in[:, :, pl.ds(pl.multiple_of(group * wide, wide), wide)].reshape(model, wide),
            preferred_element_type=F32,
        )
        left = silu(both[:, :LANE]) * both[:, LANE : 2 * LANE]
        right = silu(both[:, 2 * LANE : 3 * LANE]) * both[:, 3 * LANE :]
        h_ref[rows, pl.ds(pl.multiple_of(group * 2 * LANE, 2 * LANE), 2 * LANE)] = jnp.concatenate(
            [left.astype(BF), right.astype(BF)], axis=1
        )
        return carry

    groups = blocks // 4
    lax.fori_loop(0, groups * steps, one, 0)

    def last(m, carry):
        rows = pl.ds(pl.multiple_of(m * chunk, chunk), chunk)
        both = jnp.dot(
            x_ref[rows, :],
            w_in[:, :, groups * wide :].reshape(model, -1),
            preferred_element_type=F32,
        )
        left = silu(both[:, :LANE]) * both[:, LANE : 2 * LANE]
        gate = both[:, 2 * LANE :]
        up = pltpu.roll(gate, LANE // 2, 1)
        lane = lax.broadcasted_iota(jnp.int32, gate.shape, 1)
        right = jnp.where(lane < rest, silu(gate) * up, 0.0)
        h_ref[rows, groups * 2 * LANE :] = jnp.concatenate(
            [left.astype(BF), right.astype(BF)], axis=1
        )
        return carry

    lax.fori_loop(0, steps, last, 0)
    project(h_ref, w_out, outs, y_ref, o_sem, chunk)


def feed_rows(pieces, weights, hidden, name):
    w_in, w_out = weights
    held, model = w_out.shape
    total = sum(p.shape[0] for p in pieces)
    count = len(pieces)
    wide = 4 * LANE
    return call(
        functools.partial(feed_body, count=count, hidden=hidden),
        name,
        [jax.ShapeDtypeStruct((total // 2, model), BF)] * 2,
        [
            pltpu.VMEM((total, model), BF),
            pltpu.VMEM((total, held), BF),
            pltpu.VMEM((model // wide, total, wide), BF),
            pltpu.SemaphoreType.DMA((count,)),
            pltpu.SemaphoreType.DMA((model // wide, 2)),
        ],
        (*pieces, w_in, w_out),
        [HBM] * count + [VMEM, VMEM],
        [HBM, HBM],
        6 * total * model * hidden,
    )


def in_body(*refs, count):
    pieces = refs[:count]
    w_in, out, x_ref, x_sem = refs[count:]
    load_rows(pieces, x_ref, x_sem)
    model = x_ref.shape[1]
    half = w_in.shape[2] // 2
    for k in range(2):
        out[:, k * half : (k + 1) * half] = jnp.dot(
            x_ref[...],
            w_in[:, :, k * half : (k + 1) * half].reshape(model, half),
            preferred_element_type=F32,
        ).astype(BF)


def in_rows(pieces, w_in, name):
    model = pieces[0].shape[1]
    total = sum(p.shape[0] for p in pieces)
    count = len(pieces)
    width = w_in.shape[2]
    return call(
        functools.partial(in_body, count=count),
        name,
        jax.ShapeDtypeStruct((total, width), BF),
        [pltpu.VMEM((total, model), BF), pltpu.SemaphoreType.DMA((count,))],
        (*pieces, w_in),
        [HBM] * count + [VMEM],
        VMEM,
        2 * total * model * width,
    )


def out_body(g_ref, w_out, same, other, y_ref, o_sem):
    project(g_ref, w_out, [same, other], y_ref, o_sem, g_ref.shape[0])


def out_rows(gated, w_out, name):
    total, channels = gated.shape
    model = w_out.shape[1]
    wide = 4 * LANE
    return call(
        out_body,
        name,
        [jax.ShapeDtypeStruct((total // 2, model), BF)] * 2,
        [
            pltpu.VMEM((model // wide, total, wide), BF),
            pltpu.SemaphoreType.DMA((model // wide, 2)),
        ],
        (gated, w_out),
        [VMEM, VMEM],
        [HBM, HBM],
        2 * total * model * channels,
    )


def mixer_body(*refs, rows, channels):
    starts, far_ref, near_ref, own_ref, gates_ref, taps_ref, decay_ref, extra_ref = refs[:8]
    outs = refs[8:11]
    r_ref, b_ref, c_ref, a_ref, d_ref = refs[11:]
    total = b_ref.shape[0]
    pad = 8
    places = [
        (far_ref, outs[0], 0, 0),
        (far_ref, outs[0], 1, 4),
        (near_ref, outs[1], 0, 1),
        (near_ref, outs[1], 1, 2),
        (near_ref, outs[1], 2, 5),
        (near_ref, outs[1], 3, 6),
        (own_ref, outs[2], 0, 3),
        (own_ref, outs[2], 1, 7),
    ]
    at = [pl.multiple_of(starts[i], rows) for i in range(8)]
    r_ref[:pad, :] = jnp.zeros((pad, channels), F32)
    for ref, _, k, i in places:
        value = ref[k * rows : (k + 1) * rows, :].astype(F32)
        r_ref[pl.ds(pl.multiple_of(at[i] + pad, pad), rows), :] = value[:, :channels]
        b_ref[pl.ds(at[i], rows), :] = value[:, channels:]

    taps = taps_ref.shape[0]
    step = 128
    for m in range(total // step):
        base = m * step
        acc = r_ref[pl.ds(base + pad - taps + 1, step), :] * taps_ref[0:1, :]
        for j in range(1, taps):
            acc = acc + r_ref[pl.ds(base + pad - taps + 1 + j, step), :] * taps_ref[j : j + 1, :]
        c_ref[pl.ds(base, step), :] = acc.astype(BF)

    decay = decay_ref[...]

    def gates(m, carry):
        base = pl.multiple_of(m * step, step)
        conv = c_ref[pl.ds(base, step), :]
        pre = jnp.dot(conv, gates_ref[...], preferred_element_type=F32)
        sig = 1.0 / (1.0 + jnp.exp(-pre))
        log_a = sig[:, :channels] * decay + extra_ref[pl.ds(base, step), :]
        twice = 2.0 * log_a
        a_val = jnp.exp(log_a)
        series = -twice * (
            1.0
            + twice
            * (0.5 + twice * (1.0 / 6 + twice * (1.0 / 24 + twice * (1.0 / 120 + twice / 720.0))))
        )
        left = jnp.where(twice > -0.25, series, 1.0 - a_val * a_val)
        a_ref[pl.ds(base, step), :] = a_val
        d_ref[pl.ds(base, step), :] = jnp.sqrt(left) * sig[:, channels:] * conv.astype(F32)
        return carry

    lax.fori_loop(0, total // step, gates, 0)

    tile = 8
    group = 64
    row_in_tile = lax.broadcasted_iota(jnp.int32, (tile, channels), 0)

    def scan(m, carry):
        base = pl.multiple_of(m * group, group)
        for k in range(group // tile):
            a = a_ref[pl.ds(base + k * tile, tile), :]
            d = d_ref[pl.ds(base + k * tile, tile), :]
            for shift in (1, 2, 4):
                keep = row_in_tile >= shift
                a_prev = jnp.where(keep, pltpu.roll(a, shift, 0), 1.0)
                d_prev = jnp.where(keep, pltpu.roll(d, shift, 0), 0.0)
                d = a * d_prev + d
                a = a * a_prev
            state = a * carry + d
            carry = jnp.broadcast_to(state[tile - 1 : tile, :], (tile, channels))
            d_ref[pl.ds(base + k * tile, tile), :] = state
        return carry

    lax.fori_loop(0, total // group, scan, jnp.zeros((tile, channels), F32))

    for _, out, k, i in places:
        v = b_ref[pl.ds(at[i], rows), :]
        inner = 0.7978845608028654 * (v + 0.044715 * (v * v * v))
        gelu = 0.5 * v * (1.0 + jnp.tanh(inner))
        out[k * rows : (k + 1) * rows, :] = (gelu * d_ref[pl.ds(at[i], rows), :]).astype(BF)


def mixer_rows(starts, far, near, own, gates, taps, decay, extra, rows):
    channels = taps.shape[1]
    total = rows * 8
    return call(
        functools.partial(mixer_body, rows=rows, channels=channels),
        "mixer",
        [jax.ShapeDtypeStruct((v.shape[0], channels), BF) for v in (far, near, own)],
        [
            pltpu.VMEM((total + 8, channels), F32),
            pltpu.VMEM((total, channels), F32),
            pltpu.VMEM((total, channels), BF),
            pltpu.VMEM((total, channels), F32),
            pltpu.VMEM((total, channels), F32),
        ],
        (starts, far, near, own, gates, taps, decay, extra),
        [SMEM] + [VMEM] * 7,
        [VMEM] * 3,
        1 << 33,
    )


def normed(values, scale):
    values = values.astype(F32)
    square = jnp.mean(values * values, axis=-1, keepdims=True)
    return (values * lax.rsqrt(square + EPS) * scale).astype(BF)


def halves(x):
    return x[: x.shape[0] // 2], x[x.shape[0] // 2 :]


def block_diagonal(blocks):
    count, size, _ = blocks.shape
    return jnp.concatenate(
        [
            jnp.pad(blocks[b], ((0, 0), (b * size, (count - 1 - b) * size)))
            for b in range(count)
        ],
        axis=0,
    )


def shards(
    tokens,
    first_block_norm_scale,
    first_block_gate_matrix,
    first_block_up_matrix,
    first_block_down_matrix,
    mixer_norm_scale,
    recurrent_input_matrix,
    output_gate_projection,
    convolution_kernel,
    decay_gate_blocks,
    input_gate_blocks,
    channel_decay_weight,
    position_decay_extra,
    mixer_output_matrix,
    second_block_norm_scale,
    second_block_gate_matrix,
    second_block_up_matrix,
    second_block_down_matrix,
):
    rows = tokens.shape[0]
    hidden = first_block_gate_matrix.shape[1]
    channels = recurrent_input_matrix.shape[1]
    in_length = (2 * (hidden // LANE) + 1) * LANE

    first_weights = gathered(
        packed(pack_in, (first_block_gate_matrix.T, first_block_up_matrix.T), in_length)
    )
    mixer_weights = gathered(
        packed(
            pack_mixer,
            (recurrent_input_matrix, output_gate_projection, mixer_output_matrix),
            3 * channels,
        )
    )
    second_weights = gathered(
        packed(
            pack_feed,
            (
                second_block_gate_matrix.T,
                second_block_up_matrix.T,
                second_block_down_matrix,
            ),
            in_length + hidden,
        )
    )
    first_down = gathered_down(first_block_down_matrix)
    gates = jnp.concatenate(
        [block_diagonal(decay_gate_blocks), block_diagonal(input_gate_blocks)], axis=1
    )
    decay = (-RECURRENT_WIDTH * jax.nn.softplus(-channel_decay_weight))[None, :]
    extra = position_decay_extra[:, None]
    place = lax.axis_index("tp")
    chip, core = place // 2, place % 2
    starts = jnp.stack(
        [
            (((chip + step) % 4) * 2 + (core + other) % 2) * rows
            for other in range(2)
            for step in (2, 1, 3, 0)
        ]
    ).astype(jnp.int32)
    place = lax.axis_index("fs")
    places = jnp.stack(
        [((place // 4 + z) % 4 * 4 + (place + y) % 4) * LANE for z, y in FS_STEPS]
    ).astype(jnp.int32)

    def added(x, update, scale):
        return [(v.astype(F32) + scale * u).astype(BF) for v, u in zip(x, update)]

    def norm_both(x, scale):
        return [normed(v, scale) for v in x]

    def collected(far, near, own):
        far = far()
        got_far = along_tp(far[1], 0, 1)
        near = near(far[1])
        got_near = along_tp(near[1], 0, 1)
        far = plus(far[0], got_far).astype(BF)
        via = send_far(far)
        own = own((near[1], far))
        got_own = along_tp(own[1], 0, 1)
        near = near_sums(near[0], got_near)
        free = send_free(near)
        rest = send_rest(near, via)
        return own_sums((own[0], got_own), free, rest)

    x = halves(tokens)
    normal, gates, decay, extra, starts, places = lax.optimization_barrier(
        (norm_both(x, first_block_norm_scale), gates, decay, extra, starts, places)
    )
    near = spread_near(*normal)
    far = spread_far(near)
    own = normal + across(normal)
    near = near + across(near)
    far = far + across(far)
    blocks = in_length // LANE
    weights = placed(places, first_weights, first_down, blocks, hidden)
    total = collected(
        lambda: feed_rows(far, weights, hidden, "feed_far"),
        lambda done: feed_rows(after(near, done), weights, hidden, "feed_near"),
        lambda done: feed_rows(after(own, done), weights, hidden, "feed_own"),
    )
    x = added(x, total, 0.5)

    normal = norm_both(x, mixer_norm_scale)
    w_in, w_out = placed(places, mixer_weights, [], 2 * channels // LANE, channels)
    near = spread_near(*normal)
    far = spread_far(near)
    own = in_rows(normal + across(normal), w_in, "in_own")
    near = after(near, own)
    near = in_rows(near + across(near), w_in, "in_near")
    far = after(far, near)
    far = in_rows(far + across(far), w_in, "in_far")
    far, near, own = mixer_rows(
        starts, far, near, own, gates, convolution_kernel, decay, extra, rows
    )
    total = collected(
        lambda: out_rows(far, w_out, "out_far"),
        lambda done: out_rows(after(near, done), w_out, "out_near"),
        lambda done: out_rows(after(own, done), w_out, "out_own"),
    )
    x = added(x, total, 1.0)

    normal = norm_both(x, second_block_norm_scale)
    weights = placed(places, second_weights, [], blocks, hidden)
    near = spread_near(*normal)
    far = spread_far(near)
    own = feed_rows(normal + across(normal), weights, hidden, "feed_own")
    got_own = along_tp(own[1], 0, 1)
    near = after(near, own)
    near = feed_rows(near + across(near), weights, hidden, "feed_near")
    got_near = along_tp(near[1], 0, 1)
    far = after(far, near)
    far = feed_rows(far + across(far), weights, hidden, "feed_far")
    got_far = along_tp(far[1], 0, 1)
    near = near_sums(near[0], got_near)
    free = send_free(near)
    via = send_far(plus(far[0], got_far).astype(BF))
    rest = send_rest(near, via)
    x = added(x, own_sums((own[0], got_own), free, rest), 0.5)
    return jnp.concatenate(x, axis=0)


def solution(mesh):
    in_specs = (
        P(("fs", "tp"), None),
        P(),
        P("fs", "tp"),
        P("fs", "tp"),
        P("tp", "fs"),
        P(),
        P("fs", "tp"),
        P("fs", "tp"),
        P(None, "tp"),
        P("tp", None, None),
        P("tp", None, None),
        P("tp"),
        P("fs"),
        P("tp", "fs"),
        P(),
        P("fs", "tp"),
        P("fs", "tp"),
        P("tp", "fs"),
    )
    out_specs = P(("fs", "tp"), None)
    return jax.shard_map(shards, mesh=mesh, in_specs=in_specs, out_specs=out_specs, check_vma=False)
```

```python
import functools

import jax
import jax.numpy as jnp
from jax import lax
from jax.experimental import pallas as pl
from jax.experimental.pallas import tpu as pltpu
from jax.sharding import PartitionSpec as P


EPS = 1e-06
RECURRENT_WIDTH = 8.0
BF = jnp.bfloat16
F32 = jnp.float32
LANE = 128
CHUNK = 512
VMEM_LIMIT = 24 * 1024 * 1024


def along_tp(value, step, other_core):
    chips = lax.axis_size("tp") // 2
    pairs = [
        (x * 2 + c, ((x + step) % chips) * 2 + (c ^ other_core))
        for x in range(chips)
        for c in range(2)
    ]
    return lax.ppermute(value, "tp", pairs)


def across(values):
    return [along_tp(v, 0, 1) for v in values]


def after(values, *done):
    return lax.optimization_barrier((values, done))[0]


def spread_near(top, bottom):
    prev_top = along_tp(top, 1, 0)
    next_bottom = along_tp(bottom, -1, 0)
    prev_bottom = along_tp(bottom, 1, 0)
    next_top = along_tp(top, -1, 0)
    return [next_top, next_bottom, prev_top, prev_bottom]


def spread_far(near):
    return [along_tp(near[2], 1, 0), along_tp(near[1], -1, 0)]


def plus(a, b):
    return a.astype(F32) + b.astype(F32)


def send_far(far):
    half = far.shape[0] // 2
    return along_tp(far[:half], 1, 0), along_tp(far[half:], -1, 0)


def near_sums(same, got):
    half = same.shape[0] // 4
    return [plus(same[k * half : (k + 1) * half], got[k * half : (k + 1) * half]) for k in range(4)]


def free_rows(near):
    return near[1].astype(BF), near[2].astype(BF)


def send_free(give):
    return along_tp(give[0], 1, 0), along_tp(give[1], -1, 0)


def send_rest(near, via):
    near, via = lax.optimization_barrier((near, via))
    return (
        along_tp(plus(near[0], via[0]).astype(BF), 1, 0),
        along_tp(plus(near[3], via[1]).astype(BF), -1, 0),
    )


def own_sums(own, free, rest):
    half = own[0].shape[0] // 2
    return [
        plus(own[0][:half], own[1][:half]) + plus(free[1], rest[0]),
        plus(own[0][half:], own[1][half:]) + plus(free[0], rest[1]),
    ]


def along_fs(value, z_step, y_step):
    side = 4
    pairs = [
        (z * side + y, ((z + z_step) % side) * side + (y + y_step) % side)
        for z in range(side)
        for y in range(side)
    ]
    return lax.ppermute(value, "fs", pairs)


def ring_pieces(value, cut, move):
    prev = move(value, 1)
    nxt = move(value, -1)
    return [value, prev, nxt, move(prev[:cut], 1), move(nxt[cut:], -1)]


def gathered_down(shard):
    rows = shard.shape[0]
    cut = -(-rows // 32) * 16
    row = jnp.concatenate(ring_pieces(shard, cut, lambda v, s: along_fs(v, 0, s)), axis=0)
    return ring_pieces(row, 2 * rows, lambda v, s: along_fs(v, s, 0))


FS_STEPS = [(z, y) for z in (0, -1, 1, 2) for y in (0, -1, 1, 2)]


def pack_in(gate_ref, up_ref, out_ref):
    width, rows = gate_ref.shape
    whole = width // LANE
    rest = width - whole * LANE
    for j in range(whole):
        for k, ref in enumerate((gate_ref, up_ref)):
            block = ref[j * LANE : (j + 1) * LANE, :]
            out_ref[pl.ds((2 * j + k) * rows, rows), :] = block.T
    gap = jnp.zeros((LANE // 2 - rest, rows), BF)
    block = jnp.concatenate(
        [gate_ref[whole * LANE :, :], gap, up_ref[whole * LANE :, :], gap], axis=0
    )
    out_ref[pl.ds(2 * whole * rows, rows), :] = block.T


def pack_feed(gate_ref, up_ref, down_ref, out_ref):
    width, rows = gate_ref.shape
    pack_in(gate_ref, up_ref, out_ref)
    at = (2 * (width // LANE) + 1) * rows
    out_ref[pl.ds(at, width), :] = down_ref[...]


def pack_mixer(first_ref, second_ref, out_w_ref, out_ref):
    rows = first_ref.shape[0]
    blocks = first_ref.shape[1] // LANE
    for j in range(blocks):
        out_ref[pl.ds(j * rows, rows), :] = first_ref[:, j * LANE : (j + 1) * LANE]
        out_ref[pl.ds((blocks + j) * rows, rows), :] = second_ref[:, j * LANE : (j + 1) * LANE]
    out_ref[pl.ds(2 * blocks * rows, out_w_ref.shape[0]), :] = out_w_ref[...]


def packed(kernel, arrays, length):
    return pl.pallas_call(kernel, out_shape=jax.ShapeDtypeStruct((length, LANE), BF))(*arrays)


def gathered(shard):
    fs = lax.axis_size("fs")
    return lax.all_gather(shard, "fs", axis=0, tiled=True).reshape(fs, -1, LANE)


def row_copies(pieces, x_ref, sem):
    copies = []
    at = 0
    for i, piece in enumerate(pieces):
        rows = piece.shape[0]
        copies.append(pltpu.make_async_copy(piece, x_ref.at[pl.ds(at, rows)], sem.at[i]))
        at += rows
    return copies


def load_rows(pieces, x_ref, sem):
    copies = row_copies(pieces, x_ref, sem)
    for c in copies:
        c.start()
    for c in copies:
        c.wait()


HBM = pl.BlockSpec(memory_space=pl.ANY)
VMEM = pl.BlockSpec(memory_space=pltpu.VMEM)
SMEM = pl.BlockSpec(memory_space=pltpu.SMEM)


def call(body, outs, scratch, operands, specs, out_specs, flops):
    return pl.pallas_call(
        body,
        in_specs=specs,
        out_specs=out_specs,
        out_shape=outs,
        scratch_shapes=scratch,
        compiler_params=pltpu.CompilerParams(vmem_limit_bytes=VMEM_LIMIT),
        cost_estimate=pl.CostEstimate(flops=flops, bytes_accessed=1 << 20, transcendentals=0),
    )(*operands)


def place_copies(places_ref, w_ref, down_refs, w_in, w_out, sem, inner):
    fs = w_in.shape[0]
    blocks = w_in.shape[2] // LANE
    columns = [
        pltpu.make_async_copy(
            w_ref.at[:, pl.ds(j * LANE, LANE), :],
            w_in.at[:, :, pl.ds(j * LANE, LANE)],
            sem.at[j // 4],
        )
        for j in range(blocks)
    ]
    if not down_refs:
        shards = [w_ref.at[f, pl.ds(blocks * LANE, inner), :] for f in range(fs)]
        places = [f * LANE for f in range(fs)]
    else:
        shards = [
            ref.at[pl.ds(i * inner, inner), :]
            for ref in down_refs
            for i in range(ref.shape[0] // inner)
        ]
        places = [pl.multiple_of(places_ref[i], LANE) for i in range(fs)]
    down = [
        pltpu.make_async_copy(
            shard, w_out.at[pl.ds(0, inner), pl.ds(place, LANE)], sem.at[-(-blocks // 4)]
        )
        for shard, place in zip(shards, places)
    ]
    return columns, down


def place_body(*refs, parts, inner):
    places_ref, w_ref = refs[:2]
    w_in, w_out, sem = refs[2 + parts :]
    columns, down = place_copies(places_ref, w_ref, refs[2 : 2 + parts], w_in, w_out, sem, inner)
    for c in columns + down:
        c.start()
    for c in columns + down:
        c.wait()


def placed(places, weights, downs, blocks, inner):
    fs = weights.shape[0]
    held = -(-inner // LANE) * LANE
    weights, *downs = [pltpu.with_memory_space_constraint(w, pltpu.HBM) for w in (weights, *downs)]
    got = call(
        functools.partial(place_body, parts=len(downs), inner=inner),
        [pltpu.VMEM((fs, LANE, blocks * LANE), BF), pltpu.VMEM((held, fs * LANE), BF)],
        [pltpu.SemaphoreType.DMA((-(-blocks // 4) + 1,))],
        (places, weights, *downs),
        [SMEM] + [HBM] * (1 + len(downs)),
        [VMEM, VMEM],
        1 << 31,
    )
    return [pltpu.with_memory_space_constraint(g, pltpu.VMEM) for g in got]


def project(x_ref, w_ref, outs, y_ref, sem, chunk):
    steps = y_ref.shape[0]
    total = x_ref.shape[0]
    wide = y_ref.shape[2]

    def send(f):
        at = 0
        made = []
        for i, out in enumerate(outs):
            made.append(
                pltpu.make_async_copy(
                    y_ref.at[f, pl.ds(at, out.shape[0]), :],
                    out.at[:, pl.ds(pl.multiple_of(f * wide, wide), wide)],
                    sem.at[f, i],
                )
            )
            at += out.shape[0]
        return made

    def one(f, carry):
        columns = pl.ds(pl.multiple_of(f * wide, wide), wide)
        for m in range(total // chunk):
            y_ref[f, m * chunk : (m + 1) * chunk] = jnp.dot(
                x_ref[m * chunk : (m + 1) * chunk, :],
                w_ref[:, columns],
                preferred_element_type=F32,
            ).astype(BF)
        for copy in send(f):
            copy.start()
        return carry

    def finish(f, carry):
        for copy in send(f):
            copy.wait()
        return carry

    lax.fori_loop(0, steps, one, 0)
    lax.fori_loop(0, steps, finish, 0)


def silu(v):
    return v / (1.0 + jnp.exp(-v))


def hidden_units(x, w_in, h_ref, rows, group, rest):
    model = x.shape[1]
    wide = 4 * LANE
    blocks = w_in.shape[2] // LANE
    if isinstance(group, int) and (group + 1) * 4 > blocks:
        both = jnp.dot(
            x, w_in[:, :, group * wide :].reshape(model, -1), preferred_element_type=F32
        )
        gate = both[:, 2 * LANE :]
        up = pltpu.roll(gate, LANE // 2, 1)
        lane = lax.broadcasted_iota(jnp.int32, gate.shape, 1)
        right = jnp.where(lane < rest, silu(gate) * up, 0.0)
        at = pl.ds(group * 2 * LANE, 2 * LANE)
    else:
        both = jnp.dot(
            x,
            w_in[:, :, pl.ds(pl.multiple_of(group * wide, wide), wide)].reshape(model, wide),
            preferred_element_type=F32,
        )
        right = silu(both[:, 2 * LANE : 3 * LANE]) * both[:, 3 * LANE :]
        at = pl.ds(pl.multiple_of(group * 2 * LANE, 2 * LANE), 2 * LANE)
    left = silu(both[:, :LANE]) * both[:, LANE : 2 * LANE]
    h_ref[rows, at] = jnp.concatenate([left.astype(BF), right.astype(BF)], axis=1)


def feed_body(*refs, count, hidden):
    pieces = refs[:count]
    w_in, w_out = refs[count : count + 2]
    outs = refs[count + 2 : count + 4]
    x_ref, h_ref, y_ref, x_sem, o_sem = refs[count + 4 :]
    total = x_ref.shape[0]
    rest = hidden % LANE
    groups = w_in.shape[2] // LANE // 4
    chunk = min(CHUNK, total)
    steps = total // chunk
    load_rows(pieces, x_ref, x_sem)

    def one(i, carry):
        rows = pl.ds(pl.multiple_of(i % steps * chunk, chunk), chunk)
        hidden_units(x_ref[rows, :], w_in, h_ref, rows, i // steps, rest)
        return carry

    def last(i, carry):
        rows = pl.ds(pl.multiple_of(i * chunk, chunk), chunk)
        hidden_units(x_ref[rows, :], w_in, h_ref, rows, groups, rest)
        return carry

    lax.fori_loop(0, groups * steps, one, 0)
    lax.fori_loop(0, steps, last, 0)
    project(h_ref, w_out, outs, y_ref, o_sem, chunk)


def feed_first_body(*refs, count, parts, hidden):
    places_ref = refs[0]
    pieces = refs[1 : count + 1]
    w_ref = refs[count + 1]
    down_refs = refs[count + 2 : count + 2 + parts]
    outs = refs[count + 2 + parts : count + 4 + parts]
    w_in, w_out, x_ref, h_ref, y_ref, x_sem, o_sem, w_sem = refs[count + 4 + parts :]
    columns, down = place_copies(places_ref, w_ref, down_refs, w_in, w_out, w_sem, hidden)
    for c in columns[:4]:
        c.start()
    rows_in = row_copies(pieces, x_ref, x_sem)
    for c in rows_in + columns[4:] + down:
        c.start()
    pad = w_out.shape[0] - hidden
    w_out[hidden:, :] = jnp.zeros((pad, w_out.shape[1]), BF)
    for c in rows_in:
        c.wait()
    total = x_ref.shape[0]
    rows = pl.ds(0, total)
    for group in range(-(-len(columns) // 4)):
        for c in columns[group * 4 : group * 4 + 4]:
            c.wait()
        hidden_units(x_ref[...], w_in, h_ref, rows, group, hidden % LANE)
    for c in down:
        c.wait()
    project(h_ref, w_out, outs, y_ref, o_sem, total)


def feed_scratch(total, model, held, count):
    wide = 4 * LANE
    return [
        pltpu.VMEM((total, model), BF),
        pltpu.VMEM((total, held), BF),
        pltpu.VMEM((model // wide, total, wide), BF),
        pltpu.SemaphoreType.DMA((count,)),
        pltpu.SemaphoreType.DMA((model // wide, 2)),
    ]


def feed_first(places, pieces, weights, downs, blocks, hidden):
    fs, _, _ = weights.shape
    model = fs * LANE
    held = -(-hidden // LANE) * LANE
    total = sum(p.shape[0] for p in pieces)
    count = len(pieces)
    weights, *downs = [pltpu.with_memory_space_constraint(w, pltpu.HBM) for w in (weights, *downs)]
    same, other, w_in, w_out = call(
        functools.partial(feed_first_body, count=count, parts=len(downs), hidden=hidden),
        [jax.ShapeDtypeStruct((total // 2, model), BF)] * 2
        + [pltpu.VMEM((fs, LANE, blocks * LANE), BF), pltpu.VMEM((held, model), BF)],
        feed_scratch(total, model, held, count)
        + [pltpu.SemaphoreType.DMA((-(-blocks // 4) + 1,))],
        (places, *pieces, weights, *downs),
        [SMEM] + [HBM] * (count + 1 + len(downs)),
        [HBM, HBM, VMEM, VMEM],
        6 * total * model * hidden,
    )
    matrices = [pltpu.with_memory_space_constraint(g, pltpu.VMEM) for g in (w_in, w_out)]
    return (same, other), matrices


def feed_rows(pieces, weights, hidden):
    w_in, w_out = weights
    held, model = w_out.shape
    total = sum(p.shape[0] for p in pieces)
    count = len(pieces)
    return call(
        functools.partial(feed_body, count=count, hidden=hidden),
        [jax.ShapeDtypeStruct((total // 2, model), BF)] * 2,
        feed_scratch(total, model, held, count),
        (*pieces, w_in, w_out),
        [HBM] * count + [VMEM, VMEM],
        [HBM, HBM],
        6 * total * model * hidden,
    )


def in_body(*refs, count):
    pieces = refs[:count]
    w_in, out, x_ref, x_sem = refs[count:]
    load_rows(pieces, x_ref, x_sem)
    model = x_ref.shape[1]
    half = w_in.shape[2] // 2
    for k in range(2):
        out[:, k * half : (k + 1) * half] = jnp.dot(
            x_ref[...],
            w_in[:, :, k * half : (k + 1) * half].reshape(model, half),
            preferred_element_type=F32,
        ).astype(BF)


def in_rows(pieces, w_in):
    model = pieces[0].shape[1]
    total = sum(p.shape[0] for p in pieces)
    count = len(pieces)
    width = w_in.shape[2]
    return call(
        functools.partial(in_body, count=count),
        jax.ShapeDtypeStruct((total, width), BF),
        [pltpu.VMEM((total, model), BF), pltpu.SemaphoreType.DMA((count,))],
        (*pieces, w_in),
        [HBM] * count + [VMEM],
        VMEM,
        2 * total * model * width,
    )


def out_body(g_ref, w_out, same, other, y_ref, o_sem):
    project(g_ref, w_out, [same, other], y_ref, o_sem, g_ref.shape[0])


def out_rows(gated, w_out):
    total, channels = gated.shape
    model = w_out.shape[1]
    wide = 4 * LANE
    return call(
        out_body,
        [jax.ShapeDtypeStruct((total // 2, model), BF)] * 2,
        [
            pltpu.VMEM((model // wide, total, wide), BF),
            pltpu.SemaphoreType.DMA((model // wide, 2)),
        ],
        (gated, w_out),
        [VMEM, VMEM],
        [HBM, HBM],
        2 * total * model * channels,
    )


def mixer_body(*refs, rows, channels):
    starts, far_ref, near_ref, own_ref, gates_ref, taps_ref, decay_ref, extra_ref = refs[:8]
    outs = refs[8:11]
    r_ref, b_ref, c_ref, a_ref, d_ref = refs[11:]
    total = b_ref.shape[0]
    pad = 8
    places = [
        (far_ref, outs[0], 0, 0),
        (far_ref, outs[0], 1, 4),
        (near_ref, outs[1], 0, 1),
        (near_ref, outs[1], 1, 2),
        (near_ref, outs[1], 2, 5),
        (near_ref, outs[1], 3, 6),
        (own_ref, outs[2], 0, 3),
        (own_ref, outs[2], 1, 7),
    ]
    at = [pl.multiple_of(starts[i], rows) for i in range(8)]
    r_ref[:pad, :] = jnp.zeros((pad, channels), F32)
    for ref, _, k, i in places:
        value = ref[k * rows : (k + 1) * rows, :].astype(F32)
        r_ref[pl.ds(pl.multiple_of(at[i] + pad, pad), rows), :] = value[:, :channels]
        b_ref[pl.ds(at[i], rows), :] = value[:, channels:]

    taps = taps_ref.shape[0]
    step = 128
    for m in range(total // step):
        base = m * step
        acc = r_ref[pl.ds(base + pad - taps + 1, step), :] * taps_ref[0:1, :]
        for j in range(1, taps):
            acc = acc + r_ref[pl.ds(base + pad - taps + 1 + j, step), :] * taps_ref[j : j + 1, :]
        c_ref[pl.ds(base, step), :] = acc.astype(BF)

    decay = decay_ref[...]

    def gates(m, carry):
        base = pl.multiple_of(m * step, step)
        conv = c_ref[pl.ds(base, step), :]
        pre = jnp.dot(conv, gates_ref[...], preferred_element_type=F32)
        sig = 1.0 / (1.0 + jnp.exp(-pre))
        log_a = sig[:, :channels] * decay + extra_ref[pl.ds(base, step), :]
        twice = 2.0 * log_a
        a_val = jnp.exp(log_a)
        series = -twice * (
            1.0
            + twice
            * (0.5 + twice * (1.0 / 6 + twice * (1.0 / 24 + twice * (1.0 / 120 + twice / 720.0))))
        )
        left = jnp.where(twice > -0.25, series, 1.0 - a_val * a_val)
        a_ref[pl.ds(base, step), :] = a_val
        d_ref[pl.ds(base, step), :] = jnp.sqrt(left) * sig[:, channels:] * conv.astype(F32)
        return carry

    lax.fori_loop(0, total // step, gates, 0)

    tile = 8
    group = 64
    row_in_tile = lax.broadcasted_iota(jnp.int32, (tile, channels), 0)

    def scan(m, carry):
        base = pl.multiple_of(m * group, group)
        for k in range(group // tile):
            a = a_ref[pl.ds(base + k * tile, tile), :]
            d = d_ref[pl.ds(base + k * tile, tile), :]
            for shift in (1, 2, 4):
                keep = row_in_tile >= shift
                a_prev = jnp.where(keep, pltpu.roll(a, shift, 0), 1.0)
                d_prev = jnp.where(keep, pltpu.roll(d, shift, 0), 0.0)
                d = a * d_prev + d
                a = a * a_prev
            state = a * carry + d
            carry = jnp.broadcast_to(state[tile - 1 : tile, :], (tile, channels))
            d_ref[pl.ds(base + k * tile, tile), :] = state
        return carry

    lax.fori_loop(0, total // group, scan, jnp.zeros((tile, channels), F32))

    for _, out, k, i in places:
        v = b_ref[pl.ds(at[i], rows), :]
        inner = 0.7978845608028654 * (v + 0.044715 * (v * v * v))
        gelu = 0.5 * v * (1.0 + jnp.tanh(inner))
        out[k * rows : (k + 1) * rows, :] = (gelu * d_ref[pl.ds(at[i], rows), :]).astype(BF)


def mixer_rows(starts, far, near, own, gates, taps, decay, extra, rows):
    channels = taps.shape[1]
    total = rows * 8
    return call(
        functools.partial(mixer_body, rows=rows, channels=channels),
        [jax.ShapeDtypeStruct((v.shape[0], channels), BF) for v in (far, near, own)],
        [
            pltpu.VMEM((total + 8, channels), F32),
            pltpu.VMEM((total, channels), F32),
            pltpu.VMEM((total, channels), BF),
            pltpu.VMEM((total, channels), F32),
            pltpu.VMEM((total, channels), F32),
        ],
        (starts, far, near, own, gates, taps, decay, extra),
        [SMEM] + [VMEM] * 7,
        [VMEM] * 3,
        1 << 33,
    )


def normed(values, scale):
    values = values.astype(F32)
    square = jnp.mean(values * values, axis=-1, keepdims=True)
    return (values * lax.rsqrt(square + EPS) * scale).astype(BF)


def halves(x):
    return x[: x.shape[0] // 2], x[x.shape[0] // 2 :]


def block_diagonal(blocks):
    count, size, _ = blocks.shape
    return jnp.concatenate(
        [
            jnp.pad(blocks[b], ((0, 0), (b * size, (count - 1 - b) * size)))
            for b in range(count)
        ],
        axis=0,
    )


def shards(
    tokens,
    first_block_norm_scale,
    first_block_gate_matrix,
    first_block_up_matrix,
    first_block_down_matrix,
    mixer_norm_scale,
    recurrent_input_matrix,
    output_gate_projection,
    convolution_kernel,
    decay_gate_blocks,
    input_gate_blocks,
    channel_decay_weight,
    position_decay_extra,
    mixer_output_matrix,
    second_block_norm_scale,
    second_block_gate_matrix,
    second_block_up_matrix,
    second_block_down_matrix,
):
    rows = tokens.shape[0]
    hidden = first_block_gate_matrix.shape[1]
    channels = recurrent_input_matrix.shape[1]
    in_length = (2 * (hidden // LANE) + 1) * LANE

    first_weights = gathered(
        packed(pack_in, (first_block_gate_matrix.T, first_block_up_matrix.T), in_length)
    )
    mixer_weights = gathered(
        packed(
            pack_mixer,
            (recurrent_input_matrix, output_gate_projection, mixer_output_matrix),
            3 * channels,
        )
    )
    second_weights = gathered(
        packed(
            pack_feed,
            (
                second_block_gate_matrix.T,
                second_block_up_matrix.T,
                second_block_down_matrix,
            ),
            in_length + hidden,
        )
    )
    first_down = gathered_down(first_block_down_matrix)
    gates = jnp.concatenate(
        [block_diagonal(decay_gate_blocks), block_diagonal(input_gate_blocks)], axis=1
    )
    decay = (-RECURRENT_WIDTH * jax.nn.softplus(-channel_decay_weight))[None, :]
    extra = position_decay_extra[:, None]
    place = lax.axis_index("tp")
    chip, core = place // 2, place % 2
    starts = jnp.stack(
        [
            (((chip + step) % 4) * 2 + (core + other) % 2) * rows
            for other in range(2)
            for step in (2, 1, 3, 0)
        ]
    ).astype(jnp.int32)
    place = lax.axis_index("fs")
    places = jnp.stack(
        [((place // 4 + z) % 4 * 4 + (place + y) % 4) * LANE for z, y in FS_STEPS]
    ).astype(jnp.int32)

    def added(x, update, scale):
        return [(v.astype(F32) + scale * u).astype(BF) for v, u in zip(x, update)]

    def norm_both(x, scale):
        return [normed(v, scale) for v in x]

    def collected(far, near, own):
        far, more = far()
        got_far = along_tp(far[1], 0, 1)
        near = near(far[1], more)
        got_near = along_tp(near[1], 0, 1)
        far = plus(far[0], got_far).astype(BF)
        via = send_far(far)
        near_at = near_sums(near[0], got_near)
        give = free_rows(near_at)
        free = send_free(give)
        own = own((near[1], far, give), more)
        got_own = along_tp(own[1], 0, 1)
        rest = send_rest(near_at, via)
        return own_sums((own[0], got_own), free, rest)

    x = halves(tokens)
    normal, gates, decay, extra, starts, places = lax.optimization_barrier(
        (norm_both(x, first_block_norm_scale), gates, decay, extra, starts, places)
    )
    near = spread_near(*normal)
    far = spread_far(near)
    own = normal + across(normal)
    near = near + across(near)
    far = far + across(far)
    blocks = in_length // LANE

    def feed(far, near, own, weights, downs):
        return collected(
            lambda: feed_first(places, far, weights, downs, blocks, hidden),
            lambda done, w: feed_rows(after(near, done), w, hidden),
            lambda done, w: feed_rows(after(own, done), w, hidden),
        )

    total = feed(far, near, own, first_weights, first_down)
    x = added(x, total, 0.5)

    normal = norm_both(x, mixer_norm_scale)
    near = spread_near(*normal)
    w_in, w_out = placed(places, mixer_weights, [], 2 * channels // LANE, channels)
    far = spread_far(near)
    own = normal + across(normal)
    own = in_rows(own, w_in)
    near = after(near, own)
    near = in_rows(near + across(near), w_in)
    far = after(far, near)
    far = in_rows(far + across(far), w_in)
    far, near, own = mixer_rows(
        starts, far, near, own, gates, convolution_kernel, decay, extra, rows
    )
    total = collected(
        lambda: (out_rows(far, w_out), w_out),
        lambda done, w: out_rows(after(near, done), w),
        lambda done, w: out_rows(after(own, done), w),
    )
    x = added(x, total, 1.0)

    normal = norm_both(x, second_block_norm_scale)
    near = spread_near(*normal)
    far = spread_far(near)
    own = normal + across(normal)
    near = near + across(near)
    far = far + across(far)
    total = feed(far, near, own, second_weights, [])
    x = added(x, total, 0.5)
    return jnp.concatenate(x, axis=0)


def solution(mesh):
    in_specs = (
        P(("fs", "tp"), None),
        P(),
        P("fs", "tp"),
        P("fs", "tp"),
        P("tp", "fs"),
        P(),
        P("fs", "tp"),
        P("fs", "tp"),
        P(None, "tp"),
        P("tp", None, None),
        P("tp", None, None),
        P("tp"),
        P("fs"),
        P("tp", "fs"),
        P(),
        P("fs", "tp"),
        P("fs", "tp"),
        P("tp", "fs"),
    )
    out_specs = P(("fs", "tp"), None)

    return jax.shard_map(shards, mesh=mesh, in_specs=in_specs, out_specs=out_specs, check_vma=False)
```

```python
import functools

import jax
import jax.numpy as jnp
from jax import lax
from jax.experimental import pallas as pl
from jax.experimental.pallas import tpu as pltpu
from jax.sharding import PartitionSpec as P


EPS = 1e-06
RECURRENT_WIDTH = 8.0
BF = jnp.bfloat16
F32 = jnp.float32
LANE = 128
CHUNK = 512
VMEM_LIMIT = 24 * 1024 * 1024


def along_tp(value, step, other_core):
    chips = lax.axis_size("tp") // 2
    pairs = [
        (x * 2 + c, ((x + step) % chips) * 2 + (c ^ other_core))
        for x in range(chips)
        for c in range(2)
    ]
    return lax.ppermute(value, "tp", pairs)


def with_other(values):
    return values + [along_tp(jnp.concatenate(values, axis=0), 0, 1)]


def after(values, *done):
    return lax.optimization_barrier((values, done))[0]


def spread(top, bottom):
    prev_top = along_tp(top, 1, 0)
    next_bottom = along_tp(bottom, -1, 0)
    prev_bottom = along_tp(bottom, 1, 0)
    next_top = along_tp(top, -1, 0)
    far = [along_tp(prev_top, 1, 0), along_tp(next_bottom, -1, 0)]
    first = with_other([next_bottom, prev_top])
    second = with_other([next_top, prev_bottom])
    return with_other(far), first, second, with_other([top, bottom])


def plus(a, b):
    return a.astype(F32) + b.astype(F32)


def sums(pair):
    half = pair[0].shape[0] // 2
    return [plus(pair[0][:half], pair[1][:half]), plus(pair[0][half:], pair[1][half:])]


def send_both(values):
    return along_tp(values[0].astype(BF), 1, 0), along_tp(values[1].astype(BF), -1, 0)


def along_fs(value, z_step, y_step):
    side = 4
    pairs = [
        (z * side + y, ((z + z_step) % side) * side + (y + y_step) % side)
        for z in range(side)
        for y in range(side)
    ]
    return lax.ppermute(value, "fs", pairs)


def ring_pieces(value, cut, move):
    prev = move(value, 1)
    nxt = move(value, -1)
    return [value, prev, nxt, move(prev[:cut], 1), move(nxt[cut:], -1)]


def gathered_down(shard):
    rows = shard.shape[0]
    cut = -(-rows // 32) * 16
    row = jnp.concatenate(ring_pieces(shard, cut, lambda v, s: along_fs(v, 0, s)), axis=0)
    return ring_pieces(row, 2 * rows, lambda v, s: along_fs(v, s, 0))


RING = (0, -1, 1, 2)
FS_STEPS = [(z, y) for z in RING for y in RING]


def pack_in(gate_ref, up_ref, out_ref):
    width, rows = gate_ref.shape
    whole = width // LANE
    rest = width - whole * LANE
    for j in range(whole):
        for k, ref in enumerate((gate_ref, up_ref)):
            block = ref[j * LANE : (j + 1) * LANE, :]
            out_ref[pl.ds((2 * j + k) * rows, rows), :] = block.T
    gap = jnp.zeros((LANE // 2 - rest, rows), BF)
    block = jnp.concatenate(
        [gate_ref[whole * LANE :, :], gap, up_ref[whole * LANE :, :], gap], axis=0
    )
    out_ref[pl.ds(2 * whole * rows, rows), :] = block.T


def pack_feed(gate_ref, up_ref, down_ref, out_ref):
    width, rows = gate_ref.shape
    pack_in(gate_ref, up_ref, out_ref)
    at = (2 * (width // LANE) + 1) * rows
    out_ref[pl.ds(at, width), :] = down_ref[...]


def pack_mixer(first_ref, second_ref, out_w_ref, out_ref):
    rows = first_ref.shape[0]
    blocks = first_ref.shape[1] // LANE
    for j in range(blocks):
        out_ref[pl.ds(j * rows, rows), :] = first_ref[:, j * LANE : (j + 1) * LANE]
        out_ref[pl.ds((blocks + j) * rows, rows), :] = second_ref[:, j * LANE : (j + 1) * LANE]
    out_ref[pl.ds(2 * blocks * rows, out_w_ref.shape[0]), :] = out_w_ref[...]


def packed(kernel, arrays, length):
    return pl.pallas_call(kernel, out_shape=jax.ShapeDtypeStruct((length, LANE), BF))(*arrays)


def gathered(shard):
    fs = lax.axis_size("fs")
    return lax.all_gather(shard, "fs", axis=0, tiled=True).reshape(fs, -1, LANE)


def row_copies(pieces, x_ref, sem):
    copies = []
    at = 0
    for i, piece in enumerate(pieces):
        rows = piece.shape[0]
        copies.append(pltpu.make_async_copy(piece, x_ref.at[pl.ds(at, rows)], sem.at[i]))
        at += rows
    return copies


def load_rows(pieces, x_ref, sem):
    copies = row_copies(pieces, x_ref, sem)
    for c in copies:
        c.start()
    for c in copies:
        c.wait()


HBM = pl.BlockSpec(memory_space=pl.ANY)
VMEM = pl.BlockSpec(memory_space=pltpu.VMEM)
SMEM = pl.BlockSpec(memory_space=pltpu.SMEM)


def call(body, outs, scratch, operands, specs, out_specs, flops):
    return pl.pallas_call(
        body,
        in_specs=specs,
        out_specs=out_specs,
        out_shape=outs,
        scratch_shapes=scratch,
        compiler_params=pltpu.CompilerParams(vmem_limit_bytes=VMEM_LIMIT),
        cost_estimate=pl.CostEstimate(flops=flops, bytes_accessed=1 << 20, transcendentals=0),
    )(*operands)


def place_copies(places_ref, w_ref, down_refs, w_in, w_out, sem, inner):
    fs = w_in.shape[0]
    blocks = w_in.shape[2] // LANE
    columns = [
        pltpu.make_async_copy(
            w_ref.at[:, pl.ds(j * LANE, LANE), :],
            w_in.at[:, :, pl.ds(j * LANE, LANE)],
            sem.at[j // 4],
        )
        for j in range(blocks)
    ]
    if not down_refs:
        shards = [w_ref.at[f, pl.ds(blocks * LANE, inner), :] for f in range(fs)]
        places = [f * LANE for f in range(fs)]
    else:
        shards = [
            ref.at[pl.ds(i * inner, inner), :]
            for ref in down_refs
            for i in range(ref.shape[0] // inner)
        ]
        places = [pl.multiple_of(places_ref[i], LANE) for i in range(fs)]
    down = [
        pltpu.make_async_copy(
            shard, w_out.at[pl.ds(0, inner), pl.ds(place, LANE)], sem.at[-(-blocks // 4)]
        )
        for shard, place in zip(shards, places)
    ]
    return columns, down


def project(x_ref, w_ref, outs, y_ref, sem, chunk):
    steps = y_ref.shape[0]
    total = x_ref.shape[0]
    wide = y_ref.shape[2]

    def send(f):
        at = 0
        made = []
        for i, out in enumerate(outs):
            made.append(
                pltpu.make_async_copy(
                    y_ref.at[f, pl.ds(at, out.shape[0]), :],
                    out.at[:, pl.ds(pl.multiple_of(f * wide, wide), wide)],
                    sem.at[f, i],
                )
            )
            at += out.shape[0]
        return made

    def one(f, carry):
        columns = pl.ds(pl.multiple_of(f * wide, wide), wide)
        for m in range(total // chunk):
            y_ref[f, m * chunk : (m + 1) * chunk] = jnp.dot(
                x_ref[m * chunk : (m + 1) * chunk, :],
                w_ref[:, columns],
                preferred_element_type=F32,
            ).astype(BF)
        for copy in send(f):
            copy.start()
        return carry

    def finish(f, carry):
        for copy in send(f):
            copy.wait()
        return carry

    lax.fori_loop(0, steps, one, 0)
    lax.fori_loop(0, steps, finish, 0)


def silu(v):
    return v / (1.0 + jnp.exp(-v))


def hidden_units(x, w_in, h_ref, rows, group, rest):
    model = x.shape[1]
    wide = 4 * LANE
    blocks = w_in.shape[2] // LANE
    if isinstance(group, int) and (group + 1) * 4 > blocks:
        both = jnp.dot(
            x, w_in[:, :, group * wide :].reshape(model, -1), preferred_element_type=F32
        )
        gate = both[:, 2 * LANE :]
        up = pltpu.roll(gate, LANE // 2, 1)
        lane = lax.broadcasted_iota(jnp.int32, gate.shape, 1)
        right = jnp.where(lane < rest, silu(gate) * up, 0.0)
        at = pl.ds(group * 2 * LANE, 2 * LANE)
    else:
        both = jnp.dot(
            x,
            w_in[:, :, pl.ds(pl.multiple_of(group * wide, wide), wide)].reshape(model, wide),
            preferred_element_type=F32,
        )
        right = silu(both[:, 2 * LANE : 3 * LANE]) * both[:, 3 * LANE :]
        at = pl.ds(pl.multiple_of(group * 2 * LANE, 2 * LANE), 2 * LANE)
    left = silu(both[:, :LANE]) * both[:, LANE : 2 * LANE]
    h_ref[rows, at] = jnp.concatenate([left.astype(BF), right.astype(BF)], axis=1)


def feed_body(*refs, count, hidden):
    pieces = refs[:count]
    w_in, w_out = refs[count : count + 2]
    outs = refs[count + 2 : count + 4]
    x_ref, h_ref, y_ref, x_sem, o_sem = refs[count + 4 :]
    total = x_ref.shape[0]
    rest = hidden % LANE
    groups = w_in.shape[2] // LANE // 4
    chunk = min(CHUNK, total)
    steps = total // chunk
    load_rows(pieces, x_ref, x_sem)

    def one(i, carry):
        rows = pl.ds(pl.multiple_of(i % steps * chunk, chunk), chunk)
        hidden_units(x_ref[rows, :], w_in, h_ref, rows, i // steps, rest)
        return carry

    def last(i, carry):
        rows = pl.ds(pl.multiple_of(i * chunk, chunk), chunk)
        hidden_units(x_ref[rows, :], w_in, h_ref, rows, groups, rest)
        return carry

    lax.fori_loop(0, groups * steps, one, 0)
    lax.fori_loop(0, steps, last, 0)
    project(h_ref, w_out, outs, y_ref, o_sem, chunk)


def feed_first_body(*refs, count, parts, hidden):
    places_ref = refs[0]
    pieces = refs[1 : count + 1]
    w_ref = refs[count + 1]
    down_refs = refs[count + 2 : count + 2 + parts]
    outs = refs[count + 2 + parts : count + 4 + parts]
    w_in, w_out, x_ref, h_ref, y_ref, x_sem, o_sem, w_sem = refs[count + 4 + parts :]
    columns, down = place_copies(places_ref, w_ref, down_refs, w_in, w_out, w_sem, hidden)
    for c in columns[:4]:
        c.start()
    rows_in = row_copies(pieces, x_ref, x_sem)
    for c in rows_in + columns[4:] + down:
        c.start()
    pad = w_out.shape[0] - hidden
    w_out[hidden:, :] = jnp.zeros((pad, w_out.shape[1]), BF)
    for c in rows_in:
        c.wait()
    total = x_ref.shape[0]
    rows = pl.ds(0, total)
    for group in range(-(-len(columns) // 4)):
        for c in columns[group * 4 : group * 4 + 4]:
            c.wait()
        hidden_units(x_ref[...], w_in, h_ref, rows, group, hidden % LANE)
    for c in down:
        c.wait()
    project(h_ref, w_out, outs, y_ref, o_sem, total)


def feed_scratch(total, model, held, count):
    wide = 4 * LANE
    return [
        pltpu.VMEM((total, model), BF),
        pltpu.VMEM((total, held), BF),
        pltpu.VMEM((model // wide, total, wide), BF),
        pltpu.SemaphoreType.DMA((count,)),
        pltpu.SemaphoreType.DMA((model // wide, 2)),
    ]


def feed_first(places, pieces, weights, downs, blocks, hidden):
    fs, _, _ = weights.shape
    model = fs * LANE
    held = -(-hidden // LANE) * LANE
    total = sum(p.shape[0] for p in pieces)
    count = len(pieces)
    weights, *downs = [pltpu.with_memory_space_constraint(w, pltpu.HBM) for w in (weights, *downs)]
    pieces = pieces[:-1] + [pltpu.with_memory_space_constraint(pieces[-1], pltpu.HBM)]
    same, other, w_in, w_out = call(
        functools.partial(feed_first_body, count=count, parts=len(downs), hidden=hidden),
        [jax.ShapeDtypeStruct((total // 2, model), BF)] * 2
        + [pltpu.VMEM((fs, LANE, blocks * LANE), BF), pltpu.VMEM((held, model), BF)],
        feed_scratch(total, model, held, count)
        + [pltpu.SemaphoreType.DMA((-(-blocks // 4) + 1,))],
        (places, *pieces, weights, *downs),
        [SMEM] + [HBM] * (count + 1 + len(downs)),
        [HBM, HBM, VMEM, VMEM],
        6 * total * model * hidden,
    )
    matrices = [pltpu.with_memory_space_constraint(g, pltpu.VMEM) for g in (w_in, w_out)]
    return (same, other), matrices


def feed_rows(pieces, weights, hidden):
    w_in, w_out = weights
    held, model = w_out.shape
    total = sum(p.shape[0] for p in pieces)
    count = len(pieces)
    return call(
        functools.partial(feed_body, count=count, hidden=hidden),
        [jax.ShapeDtypeStruct((total // 2, model), BF)] * 2,
        feed_scratch(total, model, held, count),
        (*pieces, w_in, w_out),
        [HBM] * count + [VMEM, VMEM],
        [HBM, HBM],
        6 * total * model * hidden,
    )


def out_body(g_ref, w_out, same, other, y_ref, o_sem):
    project(g_ref, w_out, [same, other], y_ref, o_sem, g_ref.shape[0])


def out_rows(gated, w_out):
    total, channels = gated.shape
    model = w_out.shape[1]
    wide = 4 * LANE
    return call(
        out_body,
        [jax.ShapeDtypeStruct((total // 2, model), BF)] * 2,
        [
            pltpu.VMEM((model // wide, total, wide), BF),
            pltpu.SemaphoreType.DMA((model // wide, 2)),
        ],
        (gated, w_out),
        [VMEM, VMEM],
        [HBM, HBM],
        2 * total * model * channels,
    )


def mixer_body(*refs, count, rows, channels):
    starts = refs[0]
    pieces = refs[1 : count + 1]
    w_ref, gates_ref, taps_ref, decay_ref, extra_ref = refs[count + 1 : count + 6]
    outs = refs[count + 6 : count + 10]
    w_out, x_ref, w_in, r_ref, b_ref, c_ref, a_ref, d_ref, x_sem, w_sem = refs[count + 10 :]
    total, model = x_ref.shape
    pad = 8
    half = rows // 2
    units = [
        [(0, 0), (0, 1), (4, 0), (4, 1)],
        [(1, 1), (2, 0), (5, 1), (6, 0)],
        [(1, 0), (2, 1), (5, 0), (6, 1)],
        [(3, 0), (3, 1), (7, 0), (7, 1)],
    ]
    at = [
        pl.multiple_of(pl.multiple_of(starts[i], rows) + k * half, half)
        for group in units
        for i, k in group
    ]
    columns, down = place_copies(starts, w_ref, [], w_in, w_out, w_sem, channels)
    rows_in = []
    for i, piece in enumerate(pieces):
        for k in range(piece.shape[0] // half):
            rows_in.append(
                pltpu.make_async_copy(
                    piece.at[pl.ds(k * half, half)],
                    x_ref.at[pl.ds(at[len(rows_in)], half)],
                    x_sem.at[i],
                )
            )
    for c in columns[:4] + rows_in + columns[4:] + down:
        c.start()
    r_ref[:pad, :] = jnp.zeros((pad, channels), F32)
    for c in rows_in + columns:
        c.wait()
    chunk = min(CHUNK, total)
    for k in range(2):

        def one(m, carry):
            base = pl.multiple_of(m * chunk, chunk)
            value = jnp.dot(
                x_ref[pl.ds(base, chunk), :],
                w_in[:, :, k * channels : (k + 1) * channels].reshape(model, channels),
                preferred_element_type=F32,
            )
            value = value.astype(BF).astype(F32)
            if k == 0:
                r_ref[pl.ds(pl.multiple_of(pad + base, pad), chunk), :] = value
            else:
                b_ref[pl.ds(base, chunk), :] = value
            return carry

        lax.fori_loop(0, total // chunk, one, 0)

    taps = taps_ref.shape[0]
    step = 128
    for m in range(total // step):
        base = m * step
        acc = r_ref[pl.ds(base + pad - taps + 1, step), :] * taps_ref[0:1, :]
        for j in range(1, taps):
            acc = acc + r_ref[pl.ds(base + pad - taps + 1 + j, step), :] * taps_ref[j : j + 1, :]
        c_ref[pl.ds(base, step), :] = acc.astype(BF)

    decay = decay_ref[...]

    def gates(m, carry):
        base = pl.multiple_of(m * step, step)
        conv = c_ref[pl.ds(base, step), :]
        pre = jnp.dot(conv, gates_ref[...], preferred_element_type=F32)
        sig = 1.0 / (1.0 + jnp.exp(-pre))
        log_a = sig[:, :channels] * decay + extra_ref[pl.ds(base, step), :]
        twice = 2.0 * log_a
        a_val = jnp.exp(log_a)
        series = -twice * (
            1.0
            + twice
            * (0.5 + twice * (1.0 / 6 + twice * (1.0 / 24 + twice * (1.0 / 120 + twice / 720.0))))
        )
        left = jnp.where(twice > -0.25, series, 1.0 - a_val * a_val)
        a_ref[pl.ds(base, step), :] = a_val
        d_ref[pl.ds(base, step), :] = jnp.sqrt(left) * sig[:, channels:] * conv.astype(F32)
        return carry

    lax.fori_loop(0, total // step, gates, 0)

    tile = 8
    group = 64
    row_in_tile = lax.broadcasted_iota(jnp.int32, (tile, channels), 0)

    def scan(m, carry):
        base = pl.multiple_of(m * group, group)
        for k in range(group // tile):
            a = a_ref[pl.ds(base + k * tile, tile), :]
            d = d_ref[pl.ds(base + k * tile, tile), :]
            for shift in (1, 2, 4):
                keep = row_in_tile >= shift
                a_prev = jnp.where(keep, pltpu.roll(a, shift, 0), 1.0)
                d_prev = jnp.where(keep, pltpu.roll(d, shift, 0), 0.0)
                d = a * d_prev + d
                a = a * a_prev
            state = a * carry + d
            carry = jnp.broadcast_to(state[tile - 1 : tile, :], (tile, channels))
            d_ref[pl.ds(base + k * tile, tile), :] = state
        return carry

    lax.fori_loop(0, total // group, scan, jnp.zeros((tile, channels), F32))

    for i, start in enumerate(at):
        v = b_ref[pl.ds(start, half), :]
        inner = 0.7978845608028654 * (v + 0.044715 * (v * v * v))
        gelu = 0.5 * v * (1.0 + jnp.tanh(inner))
        value = (gelu * d_ref[pl.ds(start, half), :]).astype(BF)
        outs[i // 4][i % 4 * half : (i % 4 + 1) * half, :] = value
    for c in down:
        c.wait()


def mixer_rows(starts, pieces, weights, gates, taps, decay, extra, rows):
    channels = taps.shape[1]
    fs = weights.shape[0]
    model = fs * LANE
    total = rows * 8
    count = len(pieces)
    blocks = 2 * channels // LANE
    weights = pltpu.with_memory_space_constraint(weights, pltpu.HBM)
    *gated, w_out = call(
        functools.partial(mixer_body, count=count, rows=rows, channels=channels),
        [jax.ShapeDtypeStruct((n * rows, channels), BF) for n in (2, 2, 2, 2)]
        + [pltpu.VMEM((channels, model), BF)],
        [
            pltpu.VMEM((total, model), BF),
            pltpu.VMEM((fs, LANE, 2 * channels), BF),
            pltpu.VMEM((total + 8, channels), F32),
            pltpu.VMEM((total, channels), F32),
            pltpu.VMEM((total, channels), BF),
            pltpu.VMEM((total, channels), F32),
            pltpu.VMEM((total, channels), F32),
            pltpu.SemaphoreType.DMA((count,)),
            pltpu.SemaphoreType.DMA((-(-blocks // 4) + 1,)),
        ],
        (starts, *pieces, weights, gates, taps, decay, extra),
        [SMEM] + [HBM] * (count + 1) + [VMEM] * 4,
        [VMEM] * 5,
        1 << 34,
    )
    return gated, pltpu.with_memory_space_constraint(w_out, pltpu.VMEM)


def normed(values, scale):
    values = values.astype(F32)
    square = jnp.mean(values * values, axis=-1, keepdims=True)
    return (values * lax.rsqrt(square + EPS) * scale).astype(BF)


def halves(x):
    return x[: x.shape[0] // 2], x[x.shape[0] // 2 :]


def block_diagonal(blocks):
    count, size, _ = blocks.shape
    return jnp.concatenate(
        [
            jnp.pad(blocks[b], ((0, 0), (b * size, (count - 1 - b) * size)))
            for b in range(count)
        ],
        axis=0,
    )


def shards(
    tokens,
    first_block_norm_scale,
    first_block_gate_matrix,
    first_block_up_matrix,
    first_block_down_matrix,
    mixer_norm_scale,
    recurrent_input_matrix,
    output_gate_projection,
    convolution_kernel,
    decay_gate_blocks,
    input_gate_blocks,
    channel_decay_weight,
    position_decay_extra,
    mixer_output_matrix,
    second_block_norm_scale,
    second_block_gate_matrix,
    second_block_up_matrix,
    second_block_down_matrix,
):
    rows = tokens.shape[0]
    hidden = first_block_gate_matrix.shape[1]
    channels = recurrent_input_matrix.shape[1]
    in_length = (2 * (hidden // LANE) + 1) * LANE

    first_weights = gathered(
        packed(pack_in, (first_block_gate_matrix.T, first_block_up_matrix.T), in_length)
    )
    mixer_weights = gathered(
        packed(
            pack_mixer,
            (recurrent_input_matrix, output_gate_projection, mixer_output_matrix),
            3 * channels,
        )
    )
    second_weights = gathered(
        packed(
            pack_feed,
            (
                second_block_gate_matrix.T,
                second_block_up_matrix.T,
                second_block_down_matrix,
            ),
            in_length + hidden,
        )
    )
    first_down = gathered_down(first_block_down_matrix)
    gates = jnp.concatenate(
        [block_diagonal(decay_gate_blocks), block_diagonal(input_gate_blocks)], axis=1
    )
    decay = (-RECURRENT_WIDTH * jax.nn.softplus(-channel_decay_weight))[None, :]
    extra = position_decay_extra[:, None]
    place = lax.axis_index("tp")
    chip, core = place // 2, place % 2
    starts = jnp.stack(
        [
            (((chip + step) % 4) * 2 + (core + other) % 2) * rows
            for other in range(2)
            for step in (2, 1, 3, 0)
        ]
    ).astype(jnp.int32)
    place = lax.axis_index("fs")
    places = jnp.stack(
        [((place // 4 + z) % 4 * 4 + (place + y) % 4) * LANE for z, y in FS_STEPS]
    ).astype(jnp.int32)

    def added(x, update, scale):
        return [(v.astype(F32) + scale * u).astype(BF) for v, u in zip(x, update)]

    def norm_both(x, scale):
        return [normed(v, scale) for v in x]

    def collected(far, other_groups, compute):
        far, weights = far
        got_far = along_tp(far[1], 0, 1)
        first = compute(after(other_groups[0], far[1]), weights)
        first = first[0], along_tp(first[1], 0, 1)
        far = sums((far[0], got_far))
        via = send_both(far)
        give = [v.astype(BF) for v in sums(first)]
        free = send_both(give)
        second = compute(after(other_groups[1], first[0], far), weights)
        second = sums((second[0], along_tp(second[1], 0, 1)))
        second, via = lax.optimization_barrier((second, via))
        rest = send_both([plus(second[0], via[0]), plus(second[1], via[1])])
        own = compute(after(other_groups[2], second), weights)
        own = sums((own[0], along_tp(own[1], 0, 1)))
        return [
            own[0] + plus(free[1], rest[0]),
            own[1] + plus(free[0], rest[1]),
        ]

    x = halves(tokens)
    normal, gates, decay, extra, starts, places = lax.optimization_barrier(
        (norm_both(x, first_block_norm_scale), gates, decay, extra, starts, places)
    )
    blocks = in_length // LANE

    def feed(groups, weights, downs):
        return collected(
            feed_first(places, groups[0], weights, downs, blocks, hidden),
            groups[1:],
            lambda pieces, w: feed_rows(pieces, w, hidden),
        )

    groups = spread(*normal)
    total = feed(groups, first_weights, first_down)
    x = added(x, total, 0.5)

    normal = norm_both(x, mixer_norm_scale)
    groups = spread(*normal)
    gated, w_out = mixer_rows(
        starts,
        [p for g in groups for p in g],
        mixer_weights,
        gates,
        convolution_kernel,
        decay,
        extra,
        rows,
    )
    total = collected((out_rows(gated[0], w_out), w_out), gated[1:], lambda g, w: out_rows(g, w))
    x = added(x, total, 1.0)

    normal = norm_both(x, second_block_norm_scale)
    groups = spread(*normal)
    total = feed(groups, second_weights, [])
    x = added(x, total, 0.5)
    return jnp.concatenate(x, axis=0)


def solution(mesh):
    in_specs = (
        P(("fs", "tp"), None),
        P(),
        P("fs", "tp"),
        P("fs", "tp"),
        P("tp", "fs"),
        P(),
        P("fs", "tp"),
        P("fs", "tp"),
        P(None, "tp"),
        P("tp", None, None),
        P("tp", None, None),
        P("tp"),
        P("fs"),
        P("tp", "fs"),
        P(),
        P("fs", "tp"),
        P("fs", "tp"),
        P("tp", "fs"),
    )
    out_specs = P(("fs", "tp"), None)

    return jax.shard_map(shards, mesh=mesh, in_specs=in_specs, out_specs=out_specs, check_vma=False)
```
